128 devices in a mesh: sp: 32 (over z, y, core), tp: 4 (over x).
Axes of the slice: x: 4, y: 4, z: 4, core: 2. Of those that a mesh axis runs over, the one named last changes fastest.
Arguments:
- resid_in: bfloat16 [12288, 2048], P('sp'), may hold values from -6 to 6
- cotangent: bfloat16 [12288, 2048], P('sp'), may hold values from -2 to 2
- norm_gain: float32 [2048], replicated, may hold values from 0.1 to 1.9
- routes: int32 [12288, 2], P('sp'), may hold values from 0 to 31, all different within a row; in each aligned block of 384 rows (0 to 383, 384 to 767, ...) at most 48 rows name the same one
- route_weights: float32 [12288, 2], P('sp'), may hold values from 0.1 to 1
- gate_weight: bfloat16 [32, 2048, 1024], P('sp', None, 'tp'), may hold values from -0.125 to 0.125
- up_weight: bfloat16 [32, 2048, 1024], P('sp', None, 'tp'), may hold values from -0.125 to 0.125
- down_weight: bfloat16 [32, 1024, 2048], P('sp', 'tp'), may hold values from -0.1875 to 0.1875
- out_weight: bfloat16 [2048, 1024], P(None, 'tp'), may hold values from -0.1875 to 0.1875
- gate_b: bfloat16 [12288, 1024], P('sp', 'tp'), may hold values from -6 to 6
- gate_c: bfloat16 [12288, 1024], P('sp', 'tp'), may hold values from -6 to 6
- values_u: bfloat16 [12288, 1024], P('sp', 'tp'), may hold values from -6 to 6
- taps: float32 [3, 1024], P(None, 'tp'), may hold values from -3.5 to 3.5
Outputs:
- grad_gate_weight: float32 [32, 2048, 1024], P('sp', None, 'tp')
- grad_up_weight: float32 [32, 2048, 1024], P('sp', None, 'tp')
- grad_down_weight: float32 [32, 1024, 2048], P('sp', 'tp')
- grad_resid: bfloat16 [12288, 2048], P('sp')
- grad_out_weight: float32 [2048, 1024], P('sp', 'tp')
- grad_gate_b: bfloat16 [12288, 1024], P('sp', 'tp')
- grad_gate_c: bfloat16 [12288, 1024], P('sp', 'tp')
- grad_values: bfloat16 [12288, 1024], P('sp', 'tp')
The draws below stay inside these ranges and needn't reach their ends.
Inputs may be any that keep to these rules, and one draw needn't show every extreme that they name: `routes`: A row's 2 experts differ. In the rows of one index of sp (384 tokens) no expert is named more than 48 times, a bound that some block reaches.
All inputs are finite; a program needn't handle non-finite values.
Results may differ from the reference program's by a relative error of at most 0.024.
Values may be sent and summed in bfloat16 or wider, within the bound.
No kernel may reach another device: no remote copies, remote signals or barrier semaphores. Data moves between devices by JAX's collectives and lax.ppermute only.
A program may use at most 128 MiB of HBM per device.

```python
import math
import jax
import jax.numpy as jnp
import numpy as np
from jax import lax

D = 2048
SC = 1024
FF = 1024
TAPS = 3
TOP = 2
TOK_DEV = 384
EXPERTS = 32
CAP = 48
TOKENS = 12288
N_SP = 32
N_TP = 4


def with_spikes(entries, own_key, source, target, parts, factor):
    owner, partner = [(jnp.arange(entries.shape[axis_at]) // (entries.shape[axis_at] // parts)).reshape([-1 if axis == axis_at else 1 for axis in range(entries.ndim)]) for axis_at in (source, target)]
    chosen = jax.random.permutation(own_key, parts)[partner]
    strong = (owner == chosen) | (owner == (partner + parts // 2) % parts)
    return jnp.where(strong, factor * entries, entries)


def steps_of(key, shape, split, smallest, largest):
    factor_of, own = 1.0, jax.random.fold_in(key, 6)
    for position, blocks in split:
        draws = jnp.exp(jax.random.uniform(jax.random.fold_in(own, position), (blocks,), jnp.float32, smallest / len(split), largest / len(split)))
        factor_of = factor_of * jnp.repeat(draws, shape[position] // blocks).reshape([-1 if axis == position else 1 for axis in range(len(shape))])
    return factor_of


def deal_out(rng, own, number, rows, number_of, top, most, skew):
    sequence = jax.random.permutation(rng, number_of)
    heavy_load, common = shares(number_of, rows * top, most, skew, True), shares(number_of, rows * top, most, skew, False)
    places = jnp.arange(number_of)

    def named(tallies, rotation):
        used = int((tallies > 0).sum())
        fixed = max(1, used // 4)
        passed = fixed + (places - fixed + rotation * (used - fixed)) % max(1, number_of - fixed)
        return jnp.zeros((number_of,), jnp.int32).at[sequence[jnp.where(places < fixed, places, passed)]].set(jnp.asarray(tallies, jnp.int32))

    tallies = jnp.where(number % 4 == 0, named(heavy_load, number // 4), named(common, number - number // 4 - 1))
    mixed = jax.random.permutation(jax.random.fold_in(own, 3), number_of)
    source_of, receiver = mixed[0:number_of // 2 * 2:2], mixed[1:number_of // 2 * 2:2]
    room = jnp.minimum(tallies[source_of] - 1, most - tallies[receiver]) // 2
    room = jnp.where((source_of == sequence[0]) | (receiver == sequence[0]) | (tallies[receiver] == 0), 0, jnp.maximum(room, 0))
    passed = jax.random.randint(jax.random.fold_in(own, 4), (number_of // 2,), 0, 1 << 20) % (room + 1)
    tallies = tallies.at[source_of].add(-passed).at[receiver].add(passed)
    items = jnp.searchsorted(jnp.cumsum(tallies), jnp.arange(rows * top), side="right").astype(jnp.int32)
    listing = items.reshape(top, rows).T
    listing = listing[jax.random.permutation(jax.random.fold_in(own, 1), rows)]
    rotation = jax.random.randint(jax.random.fold_in(own, 2), (rows, 1), 0, top)
    return jnp.take_along_axis(listing, (jnp.arange(top)[None, :] + rotation) % top, axis=1)


def shares(number_of, total, reach, slope, full):
    portions = [(1 << 20) // math.isqrt(grade ** slope) + 1 for grade in range(1, number_of + 1)]
    largest = reach if full else min(reach, max(-(-total // number_of), total * portions[0] // sum(portions)))
    least = 1 if total - largest >= number_of - 1 else 0
    given, surplus = [largest] + [least] * (number_of - 1), total - largest - least * (number_of - 1)
    while surplus > 0:
        free = [i for i in range(1, number_of) if given[i] < largest] or [i for i in range(1, number_of) if given[i] < reach]
        pool, remaining = sum([portions[i] for i in free]), surplus
        for i in free:
            more = min(reach - given[i], max(1, remaining * portions[i] // pool), surplus)
            given[i] = given[i] + more
            surplus = surplus - more
    return np.array(given)


def gaussian(stream_key, extent, scale, reach, cuts=(), held_as=jnp.bfloat16):
    result = jax.random.normal(stream_key, extent, jnp.float32) * scale
    if len(cuts) > 0:
        result = steps_of(stream_key, extent, cuts, -0.22, 0.18) * result
    return jnp.clip(result, min=-reach, max=reach).astype(held_as)


def bell_draw_with(key, dims, spread, reach, pieces, heavy, held_as=jnp.bfloat16):
    drawn = spread * jax.random.normal(key, dims, jnp.float32)
    if pieces:
        drawn = drawn * steps_of(key, dims, pieces, -0.22, 0.18)
    return jnp.clip(with_spikes(drawn, jax.random.fold_in(key, 3), *heavy), -reach, reach).astype(held_as)


def setup_inputs(seed: int = 0) -> dict:
    arg_keys = jax.random.split(jax.random.key(seed), 14)
    resid_in = gaussian(arg_keys[0], (TOKENS, D), 1.0, 6.0, ((0, 32),))
    cotangent = bell_draw_with(arg_keys[1], (TOKENS, D), 0.25, 2.0, ((0, 32),), (0, 1, 32, 2.75))
    norm_gain = jnp.clip(1.0 + 0.18 * jax.random.normal(arg_keys[2], (D,), jnp.float32), 0.1, 1.9)
    routes_keys = jax.random.split(jax.random.fold_in(arg_keys[3], 1), TOKENS // TOK_DEV)
    routes_turns = jax.random.permutation(jax.random.fold_in(arg_keys[3], 3), TOKENS // TOK_DEV)
    routes = jax.vmap(lambda own, number: deal_out(jax.random.fold_in(arg_keys[3], 2), own, number, TOK_DEV, EXPERTS, TOP, CAP, 1))(routes_keys, routes_turns).reshape((TOKENS, TOP))
    route_weights = jnp.clip(0.1 + 0.9 * jax.random.uniform(arg_keys[4], (TOKENS, TOP), jnp.float32) ** steps_of(arg_keys[4], (TOKENS, TOP), ((0, 32),), -0.2, 0.2), 0.1, 1.0)
    gate_weight = gaussian(arg_keys[5], (EXPERTS, D, FF), D ** -0.5, 0.125, ((0, 32), (2, 4)))
    up_weight = gaussian(arg_keys[6], (EXPERTS, D, FF), D ** -0.5, 0.125, ((0, 32), (2, 4)))
    down_weight = gaussian(arg_keys[7], (EXPERTS, FF, D), FF ** -0.5, 0.1875, ((0, 32), (1, 4)))
    out_weight = gaussian(arg_keys[8], (D, SC), SC ** -0.5, 0.1875, ((1, 4),))
    gate_b = gaussian(arg_keys[9], (TOKENS, SC), 1.0, 6.0, ((0, 32), (1, 4)))
    gate_c = gaussian(arg_keys[10], (TOKENS, SC), 1.0, 6.0, ((0, 32), (1, 4)))
    values_u = gaussian(arg_keys[11], (TOKENS, SC), 1.0, 6.0, ((0, 32), (1, 4)))
    taps = gaussian(arg_keys[12], (TAPS, SC), TAPS ** -0.5, 3.5, ((1, 4),), jnp.float32)
    return dict(resid_in=resid_in, cotangent=cotangent, norm_gain=norm_gain, routes=routes, route_weights=route_weights, gate_weight=gate_weight, up_weight=up_weight, down_weight=down_weight, out_weight=out_weight, gate_b=gate_b, gate_c=gate_c, values_u=values_u, taps=taps)


norm_eps = 1e-06

def expert_pass(entry_rows, entry_cots, entry_weights, gate_mat, up_mat, down_mat):
    f32 = jnp.float32
    bf16 = jnp.bfloat16
    gate_pre = jnp.dot(entry_rows, gate_mat, preferred_element_type=f32)
    up_pre = jnp.dot(entry_rows, up_mat, preferred_element_type=f32)
    logistic = jax.nn.sigmoid(gate_pre)
    activated = gate_pre * logistic
    hidden = (activated * up_pre * entry_weights[:, None]).astype(bf16)
    grad_down = jnp.dot(hidden.T, entry_cots, preferred_element_type=f32)
    dhidden = jnp.dot(entry_cots, down_mat.T, preferred_element_type=f32) * entry_weights[:, None]
    dgate = (dhidden * up_pre * logistic * (1.0 + gate_pre * (1.0 - logistic))).astype(bf16)
    dup = (dhidden * activated).astype(bf16)
    grad_gate = jnp.dot(entry_rows.T, dgate, preferred_element_type=f32)
    grad_up = jnp.dot(entry_rows.T, dup, preferred_element_type=f32)
    quarter = gate_mat.shape[1] // N_TP
    summed = jnp.zeros((entry_rows.shape[0], entry_rows.shape[1]), f32)
    for lane_index in range(N_TP):
        lower = lane_index * quarter
        upper = lower + quarter
        partial_sum = jnp.dot(dgate[:, lower:upper], gate_mat[:, lower:upper].T, preferred_element_type=f32) + jnp.dot(dup[:, lower:upper], up_mat[:, lower:upper].T, preferred_element_type=f32)
        summed = summed + lax.optimization_barrier(partial_sum.astype(bf16)).astype(f32)
    return (grad_gate, grad_up, grad_down, summed.astype(bf16))

def reference(resid_in, cotangent, norm_gain, routes, route_weights, gate_weight, up_weight, down_weight, out_weight, gate_b, gate_c, values_u, taps):
    f32 = jnp.float32
    bf16 = jnp.bfloat16
    token_total = resid_in.shape[0]
    resid_wide = resid_in.astype(f32)
    inv_rms = lax.rsqrt(lax.optimization_barrier(jnp.mean(resid_wide * resid_wide, axis=1, keepdims=True)) + norm_eps)
    normed = (resid_wide * inv_rms * norm_gain).astype(bf16)
    flat_routes = routes.reshape(-1).astype(jnp.int32)
    flat_weights = route_weights.reshape(-1)
    slot_total = N_SP * CAP

    def one_expert(expert_id):
        chosen = flat_routes == expert_id
        found = jnp.nonzero(chosen, size=slot_total, fill_value=0)[0].astype(jnp.int32)
        how_many = jnp.sum(chosen.astype(jnp.int32))
        is_valid = jnp.arange(slot_total, dtype=jnp.int32) < how_many
        owners = found // 2
        entry_weights = jnp.where(is_valid, flat_weights[found], jnp.zeros((), f32))
        grads = expert_pass(normed[owners], cotangent[owners], entry_weights, gate_weight[expert_id], up_weight[expert_id], down_weight[expert_id])
        targets = jnp.where(is_valid, found, 2 * token_total).astype(jnp.int32)
        return (grads[0], grads[1], grads[2], grads[3], targets)
    grad_gate_weight, grad_up_weight, grad_down_weight, slot_rows, targets = lax.map(one_expert, jnp.arange(EXPERTS, dtype=jnp.int32))
    slot_grads = jnp.zeros((2 * token_total + 1, D), f32).at[targets.reshape(-1)].add(slot_rows.reshape(-1, D).astype(f32))
    paired = slot_grads[:2 * token_total].reshape(token_total, 2, D)
    dnormed = paired[:, 0] + paired[:, 1]
    scaled = dnormed * norm_gain
    resid_grad = cotangent.astype(f32) + inv_rms * scaled - resid_wide * inv_rms ** 3 * lax.optimization_barrier(jnp.mean(scaled * resid_wide, axis=1, keepdims=True))
    grad_resid = resid_grad.astype(bf16)
    mixed = gate_c.astype(f32) * values_u.astype(f32)
    padded = jnp.pad(mixed, ((2, 0), (0, 0)))
    conv = taps[0] * padded[:-2] + taps[1] * padded[1:-1] + taps[2] * padded[2:]
    merged = (gate_b.astype(f32) * conv).astype(bf16)
    grad_out_weight = jnp.dot(grad_resid.T, merged, preferred_element_type=f32)
    dmerged = jnp.dot(grad_resid, out_weight, preferred_element_type=f32)
    grad_gate_b = (dmerged * conv).astype(bf16)
    dconv = dmerged * gate_b.astype(f32)
    padded_grad = jnp.pad(dconv, ((0, 2), (0, 0)))
    dmixed = taps[2] * padded_grad[:-2] + taps[1] * padded_grad[1:-1] + taps[0] * padded_grad[2:]
    grad_gate_c = (dmixed * values_u.astype(f32)).astype(bf16)
    grad_values = (dmixed * gate_c.astype(f32)).astype(bf16)
    return (grad_gate_weight, grad_up_weight, grad_down_weight, grad_resid, grad_out_weight, grad_gate_b, grad_gate_c, grad_values)
```

```python
import jax
import jax.numpy as jnp
from jax import lax
from jax.sharding import PartitionSpec as P

norm_eps = 1e-06
chunks = 2
f32 = jnp.float32
bf16 = jnp.bfloat16


def passed_along(array, axis, by):
    size = lax.axis_size(axis)
    pairs = [(i, i + by) for i in range(size) if 0 <= i + by < size]
    return lax.ppermute(array, axis, pairs)


def turned(array, by):
    size = lax.axis_size("tp")
    return lax.ppermute(array, "tp", [(i, (i + by) % size) for i in range(size)])


def exchanged(array):
    return lax.all_to_all(array, "sp", split_axis=0, concat_axis=0, tiled=True)


def ring_gather(piece):
    half = piece.shape[0] // 2
    prev = turned(piece, 1)
    nxt = turned(piece, -1)
    far_top = turned(prev[:half], 1)
    far_low = turned(nxt[half:], -1)
    return prev, nxt, far_top, far_low


def placed_columns(lane, pieces, width):
    piece, (prev, nxt, far_top, far_low) = pieces
    half = piece.shape[0] // 2
    size = piece.shape[1]
    lanes = width // size
    whole = jnp.zeros((piece.shape[0], width), piece.dtype)
    whole = lax.dynamic_update_slice(whole, piece, (0, lane * size))
    whole = lax.dynamic_update_slice(whole, prev, (0, ((lane + lanes - 1) % lanes) * size))
    whole = lax.dynamic_update_slice(whole, nxt, (0, ((lane + 1) % lanes) * size))
    far = ((lane + 2) % lanes) * size
    whole = lax.dynamic_update_slice(whole, far_top, (0, far))
    return lax.dynamic_update_slice(whole, far_low, (half, far))


def ring_scatter(part_of):
    far = part_of(2)
    half = far.shape[0] // 2
    from_prev = turned(far[:half], 1)
    from_next = turned(far[half:], -1)
    ahead = part_of(1)
    behind = part_of(3)
    ahead = jnp.concatenate(
        [(ahead[:half].astype(f32) + from_prev.astype(f32)).astype(bf16), ahead[half:]], axis=0
    )
    behind = jnp.concatenate(
        [behind[:half], (behind[half:].astype(f32) + from_next.astype(f32)).astype(bf16)], axis=0
    )
    from_prev = turned(ahead, 1)
    from_next = turned(behind, -1)
    own = part_of(0)
    return (own.astype(f32) + from_prev.astype(f32) + from_next.astype(f32)).astype(bf16)


def on_device(
    resid_in,
    cotangent,
    norm_gain,
    routes,
    route_weights,
    gate_weight,
    up_weight,
    down_weight,
    out_weight,
    gate_b,
    gate_c,
    values_u,
    taps,
):
    token_count, model_width = resid_in.shape
    groups = lax.axis_size("sp")
    lanes = lax.axis_size("tp")
    lane = lax.axis_index("tp")
    expert_total = gate_weight.shape[0] * groups
    capacity = 4 * token_count // expert_total
    slots = expert_total * capacity
    quarter = model_width // lanes
    gate_mat, up_mat, down_mat = gate_weight[0], up_weight[0], down_weight[0]

    expert_ids = jnp.arange(expert_total, dtype=jnp.int32)[:, None]
    first = routes[:, 0][None, :] == expert_ids
    second = routes[:, 1][None, :] == expert_ids
    named = first | second
    order = jnp.arange(token_count, dtype=jnp.int32)
    earlier_mask = (order[:, None] < order[None, :]).astype(bf16)
    rank = jnp.dot(named.astype(bf16), earlier_mask, preferred_element_type=f32).astype(jnp.int32)
    rank = jnp.where(named, rank, -1)
    in_slot = rank[:, None, :] == jnp.arange(capacity, dtype=jnp.int32)[None, :, None]
    weight_of = jnp.where(first, route_weights[:, 0][None, :], 0.0) + jnp.where(
        second, route_weights[:, 1][None, :], 0.0
    )
    slot_weight = jnp.sum(jnp.where(in_slot, weight_of[:, None, :], 0.0), axis=2).reshape(slots, 1)
    chooser = in_slot.astype(bf16).reshape(slots, token_count)

    resid_wide = resid_in.astype(f32)
    inv_rms = lax.rsqrt(jnp.mean(resid_wide * resid_wide, axis=1, keepdims=True) + norm_eps)
    resid_part = lax.dynamic_slice_in_dim(resid_in, lane * quarter, quarter, axis=1)
    gain_part = lax.dynamic_slice_in_dim(norm_gain, lane * quarter, quarter, axis=0)
    normed_part = (resid_part.astype(f32) * inv_rms * gain_part).astype(bf16)
    sent_rows = jnp.dot(chooser, normed_part, preferred_element_type=f32).astype(bf16)
    got_part = exchanged(sent_rows.reshape(groups, capacity, quarter)).reshape(slots, quarter)
    sent_cots = (
        jnp.dot(chooser, cotangent, preferred_element_type=f32) * slot_weight
    ).astype(bf16)
    entry_cots = exchanged(sent_cots.reshape(groups, capacity, model_width)).reshape(
        slots, model_width
    )
    entry_rows = placed_columns(lane, (got_part, ring_gather(got_part)), model_width)

    mixed = gate_c.astype(f32) * values_u.astype(f32)
    earlier = passed_along(mixed[-2:], "sp", 1)

    gate_pre = jnp.dot(entry_rows, gate_mat, preferred_element_type=f32)
    up_pre = jnp.dot(entry_rows, up_mat, preferred_element_type=f32)
    logistic = jax.nn.sigmoid(gate_pre)
    activated = gate_pre * logistic
    hidden = (activated * up_pre).astype(bf16)
    dhidden = jnp.einsum("rd,fd->rf", entry_cots, down_mat, preferred_element_type=f32)
    dgate = (dhidden * up_pre * logistic * (1.0 + gate_pre * (1.0 - logistic))).astype(bf16)
    dup = (dhidden * activated).astype(bf16)
    dboth = jnp.concatenate([dgate, dup], axis=1)
    both_mat = jnp.concatenate([gate_mat, up_mat], axis=1)

    width = quarter // chunks
    grad_pieces = []
    for chunk in range(chunks):

        def part_of(further, chunk=chunk):
            at = ((lane + further) % lanes) * quarter + chunk * width
            mat = lax.dynamic_slice_in_dim(both_mat, at, width, axis=0)
            return jnp.einsum("rf,df->rd", dboth, mat, preferred_element_type=f32).astype(bf16)

        summed = ring_scatter(part_of)
        returned = exchanged(summed.reshape(groups, capacity, width)).reshape(slots, width)
        pair_sum = jnp.einsum("st,sd->td", chooser, returned, preferred_element_type=f32)
        grad_pieces.append(pair_sum.astype(bf16))
    grad_piece = jnp.concatenate(grad_pieces, axis=1)
    dnormed = placed_columns(lane, (grad_piece, ring_gather(grad_piece)), model_width).astype(f32)

    grad_down = jnp.einsum("rf,rd->fd", hidden, entry_cots, preferred_element_type=f32)
    grad_gate = jnp.einsum("rd,rf->df", entry_rows, dgate, preferred_element_type=f32)
    grad_up = jnp.einsum("rd,rf->df", entry_rows, dup, preferred_element_type=f32)

    scaled = dnormed * norm_gain
    resid_grad = (
        cotangent.astype(f32)
        + inv_rms * scaled
        - resid_wide * inv_rms**3 * jnp.mean(scaled * resid_wide, axis=1, keepdims=True)
    )
    grad_resid = resid_grad.astype(bf16)
    extended = jnp.concatenate([earlier, mixed], axis=0)
    conv = (
        taps[0] * extended[:token_count]
        + taps[1] * extended[1 : token_count + 1]
        + taps[2] * extended[2 : token_count + 2]
    )
    merged = (gate_b.astype(f32) * conv).astype(bf16)
    out_parts = jnp.einsum("td,tc->dc", grad_resid, merged, preferred_element_type=f32).astype(bf16)
    out_tiles = exchanged(out_parts.reshape(groups, model_width // groups, -1))
    grad_out_weight = jnp.sum(out_tiles.astype(f32), axis=0)
    dmerged = jnp.dot(grad_resid, out_weight, preferred_element_type=f32)
    grad_gate_b = (dmerged * conv).astype(bf16)
    dconv = dmerged * gate_b.astype(f32)
    later = passed_along(dconv[:2], "sp", -1)
    extended_grad = jnp.concatenate([dconv, later], axis=0)
    dmixed = (
        taps[2] * extended_grad[:token_count]
        + taps[1] * extended_grad[1 : token_count + 1]
        + taps[0] * extended_grad[2 : token_count + 2]
    )
    grad_gate_c = (dmixed * values_u.astype(f32)).astype(bf16)
    grad_values = (dmixed * gate_c.astype(f32)).astype(bf16)
    return (
        grad_gate[None],
        grad_up[None],
        grad_down[None],
        grad_resid,
        grad_out_weight,
        grad_gate_b,
        grad_gate_c,
        grad_values,
    )


def solution(mesh):
    placed = (
        P("sp", None),
        P("sp", None),
        P(),
        P("sp", None),
        P("sp", None),
        P("sp", None, "tp"),
        P("sp", None, "tp"),
        P("sp", "tp", None),
        P(None, "tp"),
        P("sp", "tp"),
        P("sp", "tp"),
        P("sp", "tp"),
        P(None, "tp"),
    )
    return jax.shard_map(
        on_device,
        mesh=mesh,
        in_specs=placed,
        out_specs=(
            P("sp", None, "tp"),
            P("sp", None, "tp"),
            P("sp", "tp", None),
            P("sp", None),
            P("sp", "tp"),
            P("sp", "tp"),
            P("sp", "tp"),
            P("sp", "tp"),
        ),
        check_vma=False,
    )
```

```python
import jax
import jax.numpy as jnp
from jax import lax
from jax.experimental import pallas as pl
from jax.experimental.pallas import tpu as pltpu
from jax.sharding import PartitionSpec as P

norm_eps = 1e-06
direct_width = 128
f32 = jnp.float32
bf16 = jnp.bfloat16


def passed_along(array, axis, by):
    size = lax.axis_size(axis)
    pairs = [(i, i + by) for i in range(size) if 0 <= i + by < size]
    return lax.ppermute(array, axis, pairs)


def turned(array, by):
    size = lax.axis_size("tp")
    return lax.ppermute(array, "tp", [(i, (i + by) % size) for i in range(size)])


def exchanged(array):
    return lax.all_to_all(array, "sp", split_axis=0, concat_axis=0, tiled=True)


def ring_gather(piece):
    half = piece.shape[0] // 2
    prev = turned(piece, 1)
    nxt = turned(piece, -1)
    far_top = turned(prev[:half], 1)
    far_low = turned(nxt[half:], -1)
    return prev, nxt, far_top, far_low


def placed_columns(lane, pieces, width):
    piece, (prev, nxt, far_top, far_low) = pieces
    half = piece.shape[0] // 2
    size = piece.shape[1]
    lanes = width // size
    whole = jnp.zeros((piece.shape[0], width), piece.dtype)
    whole = lax.dynamic_update_slice(whole, piece, (0, lane * size))
    whole = lax.dynamic_update_slice(whole, prev, (0, ((lane + lanes - 1) % lanes) * size))
    whole = lax.dynamic_update_slice(whole, nxt, (0, ((lane + 1) % lanes) * size))
    far = ((lane + 2) % lanes) * size
    whole = lax.dynamic_update_slice(whole, far_top, (0, far))
    return lax.dynamic_update_slice(whole, far_low, (half, far))


def lane_gather(piece):
    others = []
    for way in (1, -1, 2):
        others.append(turned(piece, way))
    return piece, *others


lane_steps = (0, -1, 1, 2)


def finish_kernel(lane_ref, *refs):
    wide_refs, narrow_refs, direct_refs = refs[:4], refs[4:8], refs[8:12]
    cot_ref, resid_ref, gain_ref, out_ref, grad_ref = refs[12:]
    width = grad_ref.shape[1]
    quarter = width // 4
    wide = wide_refs[0].shape[1]
    for step, wide_ref, narrow_ref in zip(lane_steps, wide_refs, narrow_refs):
        start = ((lane_ref[0] + (4 + step)) % 4) * quarter
        grad_ref[:, pl.ds(pl.multiple_of(start, 128), wide)] = wide_ref[...].astype(f32)
        grad_ref[:, pl.ds(pl.multiple_of(start + wide, 128), direct_width)] = narrow_ref[
            ...
        ].astype(f32)
    direct = sum(ref[...].astype(f32) for ref in direct_refs)
    for place in range(4):
        end = (place + 1) * quarter
        grad_ref[:, end - direct_width : end] = direct[
            :, place * direct_width : (place + 1) * direct_width
        ]
    resid = resid_ref[...].astype(f32)
    inv_rms = lax.rsqrt(jnp.mean(resid * resid, axis=1, keepdims=True) + norm_eps)
    scaled = grad_ref[...] * gain_ref[...]
    inner = jnp.mean(scaled * resid, axis=1, keepdims=True)
    out_ref[...] = (
        cot_ref[...].astype(f32) + inv_rms * scaled - resid * (inv_rms**3 * inner)
    ).astype(bf16)


def finish(lane, pieces, cotangent, resid_in, norm_gain):
    tokens, width = cotangent.shape
    block = 64

    def rows(array):
        return pl.BlockSpec((block, array.shape[1]), lambda i, _: (i, 0))

    gain = norm_gain.reshape(1, width)
    return pl.pallas_call(
        finish_kernel,
        grid_spec=pltpu.PrefetchScalarGridSpec(
            num_scalar_prefetch=1,
            grid=(tokens // block,),
            in_specs=[rows(x) for x in (*pieces, cotangent, resid_in)]
            + [pl.BlockSpec((1, width), lambda i, _: (0, 0))],
            out_specs=pl.BlockSpec((block, width), lambda i, _: (i, 0)),
            scratch_shapes=[pltpu.VMEM((block, width), f32)],
        ),
        out_shape=jax.ShapeDtypeStruct((tokens, width), bf16),
    )(lane.reshape(1), *pieces, cotangent, resid_in, gain)


def weighted_kernel(chooser_ref, cot_ref, weight_ref, out_ref):
    rows = jnp.dot(chooser_ref[...], cot_ref[...], preferred_element_type=f32)
    out_ref[...] = (rows * weight_ref[...]).astype(bf16)


def weighted_rows(chooser, cotangent, slot_weight):
    slots, tokens = chooser.shape
    width = cotangent.shape[1]
    block, part = 256, 512
    return pl.pallas_call(
        weighted_kernel,
        grid=(width // part, slots // block),
        in_specs=[
            pl.BlockSpec((block, tokens), lambda j, i: (i, 0)),
            pl.BlockSpec((tokens, part), lambda j, i: (0, j)),
            pl.BlockSpec((block, 1), lambda j, i: (i, 0)),
        ],
        out_specs=pl.BlockSpec((block, part), lambda j, i: (i, j)),
        out_shape=jax.ShapeDtypeStruct((slots, width), bf16),
    )(chooser, cotangent, slot_weight)


along_last = (((1,), (1,)), ((), ()))


def expert_kernel(lane_ref, gate_ref, up_ref, cot_ref, down_ref, gmat_ref, umat_ref, *outs):
    hidden_ref, dgate_ref, dup_ref, own_ref, direct_ref = outs[:5]
    further_refs = (outs[5:8], outs[8:11], outs[11:14])
    quarter = gmat_ref.shape[0] // 4
    dhidden = lax.dot_general(
        cot_ref[...], down_ref[...], along_last, preferred_element_type=f32
    )
    gate_pre = gate_ref[...]
    up_pre = up_ref[...]
    logistic = jax.nn.sigmoid(gate_pre)
    activated = gate_pre * logistic
    hidden_ref[...] = (activated * up_pre).astype(bf16)
    dgate = (dhidden * up_pre * logistic * (1.0 + gate_pre * (1.0 - logistic))).astype(bf16)
    dup = (dhidden * activated).astype(bf16)
    dgate_ref[...] = dgate
    dup_ref[...] = dup
    for further in range(4):
        place = (lane_ref[0] + further) % 4
        at = pl.ds(pl.multiple_of(place * quarter, 128), quarter)
        part = lax.dot_general(
            dgate, gmat_ref[at, :], along_last, preferred_element_type=f32
        ) + lax.dot_general(dup, umat_ref[at, :], along_last, preferred_element_type=f32)
        part = part.astype(bf16)
        direct_ref[:, pl.ds(pl.multiple_of(place * direct_width, 128), direct_width)] = part[
            :, quarter - direct_width :
        ]
        if further == 0:
            own_ref[...] = part[:, : quarter - direct_width]
        else:
            for i, ref in enumerate(further_refs[further - 1]):
                ref[...] = part[:, i * direct_width : (i + 1) * direct_width]


def expert_grads(lane, gate_pre, up_pre, entry_cots, down_mat, gate_mat, up_mat):
    slots, width = entry_cots.shape
    inner = gate_pre.shape[1]
    quarter = width // 4
    block = 256

    def rows(size):
        return pl.BlockSpec((block, size), lambda i, _: (i, 0))

    def whole(array):
        return pl.BlockSpec(array.shape, lambda i, _: (0, 0))

    sizes = [inner] * 3 + [quarter - direct_width, 4 * direct_width] + [direct_width] * 9
    return pl.pallas_call(
        expert_kernel,
        grid_spec=pltpu.PrefetchScalarGridSpec(
            num_scalar_prefetch=1,
            grid=(slots // block,),
            in_specs=[rows(inner), rows(inner), rows(width)]
            + [whole(x) for x in (down_mat, gate_mat, up_mat)],
            out_specs=[rows(size) for size in sizes],
        ),
        out_shape=[jax.ShapeDtypeStruct((slots, size), bf16) for size in sizes],
    )(lane.reshape(1), gate_pre, up_pre, entry_cots, down_mat, gate_mat, up_mat)


def on_device(
    resid_in,
    cotangent,
    norm_gain,
    routes,
    route_weights,
    gate_weight,
    up_weight,
    down_weight,
    out_weight,
    gate_b,
    gate_c,
    values_u,
    taps,
):
    token_count, model_width = resid_in.shape
    groups = lax.axis_size("sp")
    lanes = lax.axis_size("tp")
    lane = lax.axis_index("tp")
    expert_total = gate_weight.shape[0] * groups
    capacity = 4 * token_count // expert_total
    slots = expert_total * capacity
    quarter = model_width // lanes
    gate_mat, up_mat, down_mat = gate_weight[0], up_weight[0], down_weight[0]

    expert_ids = jnp.arange(expert_total, dtype=jnp.int32)[:, None]
    first = routes[:, 0][None, :] == expert_ids
    second = routes[:, 1][None, :] == expert_ids
    named = first | second
    order = jnp.arange(token_count, dtype=jnp.int32)
    earlier_mask = (order[:, None] < order[None, :]).astype(bf16)
    rank = jnp.dot(named.astype(bf16), earlier_mask, preferred_element_type=f32).astype(jnp.int32)
    rank = jnp.where(named, rank, -1)
    in_slot = rank[:, None, :] == jnp.arange(capacity, dtype=jnp.int32)[None, :, None]
    weight_of = jnp.where(first, route_weights[:, 0][None, :], 0.0) + jnp.where(
        second, route_weights[:, 1][None, :], 0.0
    )
    slot_weight = jnp.sum(jnp.where(in_slot, weight_of[:, None, :], 0.0), axis=2).reshape(slots, 1)
    chooser = in_slot.astype(bf16).reshape(slots, token_count)
    spread = (jnp.arange(slots, dtype=jnp.int32) // capacity)[None, :] == expert_ids
    slot_ranks = jnp.einsum(
        "et,es->ts", rank.astype(bf16), spread.astype(bf16), preferred_element_type=f32
    )
    slot_order = (jnp.arange(slots, dtype=jnp.int32) % capacity).astype(f32)
    token_chooser = (slot_ranks == slot_order[None, :]).astype(bf16)

    resid_wide = resid_in.astype(f32)
    inv_rms = lax.rsqrt(jnp.mean(resid_wide * resid_wide, axis=1, keepdims=True) + norm_eps)
    resid_part = lax.dynamic_slice_in_dim(resid_in, lane * quarter, quarter, axis=1)
    gain_part = lax.dynamic_slice_in_dim(norm_gain, lane * quarter, quarter, axis=0)
    normed_part = (resid_part.astype(f32) * inv_rms * gain_part).astype(bf16)
    sent_rows = jnp.dot(chooser, normed_part, preferred_element_type=f32).astype(bf16)
    got_part = exchanged(sent_rows.reshape(groups, capacity, quarter)).reshape(slots, quarter)
    sent_cots = weighted_rows(chooser, cotangent, slot_weight)
    entry_cots = exchanged(sent_cots.reshape(groups, capacity, model_width)).reshape(
        slots, model_width
    )
    entry_rows = placed_columns(lane, (got_part, ring_gather(got_part)), model_width)

    mixed = gate_c.astype(f32) * values_u.astype(f32)
    earlier = passed_along(mixed[-2:], "sp", 1)

    gate_pre = jnp.dot(entry_rows, gate_mat, preferred_element_type=f32)
    up_pre = jnp.dot(entry_rows, up_mat, preferred_element_type=f32)
    hidden, dgate, dup, own, direct, *others = expert_grads(
        lane, gate_pre, up_pre, entry_cots, down_mat, gate_mat, up_mat
    )
    a_ahead, b_ahead, c_ahead, a_far, b_far, c_far, a_behind, b_behind, c_behind = others

    def back(array):
        return exchanged(array.reshape(groups, capacity, -1)).reshape(slots, -1)

    def per_token(array):
        return jnp.dot(token_chooser, array, preferred_element_type=f32).astype(bf16)

    def plus(*arrays):
        return sum(array.astype(f32) for array in arrays).astype(bf16)

    a_far = turned(a_far, 1)
    b_far = turned(b_far, -1)
    a_next = turned(a_behind, -1)
    b_prev = turned(b_ahead, 1)
    direct = per_token(back(direct))
    a_prev = turned(plus(a_ahead, a_far), 1)
    b_next = turned(plus(b_behind, b_far), -1)
    c_far, c_behind, a_far = lax.optimization_barrier((c_far, c_behind, a_far))
    c_far = turned(c_far, 1)
    c_next = turned(c_behind, -1)
    c_prev = turned(plus(c_ahead, c_far), 1)
    pair = 2 * direct_width
    wide = jnp.concatenate(
        [
            plus(own[:, :direct_width], a_prev, a_next),
            plus(own[:, direct_width:pair], b_prev, b_next),
        ],
        axis=1,
    )
    own_last = own[:, pair:]
    wide, direct, own_last, hidden = lax.optimization_barrier((wide, direct, own_last, hidden))
    grad_down = jnp.einsum("rf,rd->fd", hidden, entry_cots, preferred_element_type=f32)
    direct_parts = lane_gather(direct)
    wide = per_token(back(wide))
    narrow = plus(own_last, c_prev, c_next)
    narrow, wide = lax.optimization_barrier((narrow, wide))
    wide_parts = lane_gather(wide)
    narrow_parts = lane_gather(per_token(back(narrow)))
    pieces = (*wide_parts, *narrow_parts, *direct_parts)
    grad_resid = finish(lane, pieces, cotangent, resid_in, norm_gain)

    extended = jnp.concatenate([earlier, mixed], axis=0)
    conv = (
        taps[0] * extended[:token_count]
        + taps[1] * extended[1 : token_count + 1]
        + taps[2] * extended[2 : token_count + 2]
    )
    merged = (gate_b.astype(f32) * conv).astype(bf16)
    out_parts = jnp.einsum("td,tc->dc", grad_resid, merged, preferred_element_type=f32).astype(bf16)
    out_tiles = exchanged(out_parts.reshape(groups, model_width // groups, -1))
    grad_out_weight = jnp.sum(out_tiles.astype(f32), axis=0)
    dgate, out_parts = lax.optimization_barrier((dgate, out_parts))
    grad_gate = jnp.einsum("rd,rf->df", entry_rows, dgate, preferred_element_type=f32)
    late_resid, grad_gate, dup = lax.optimization_barrier((grad_resid, grad_gate, dup))
    grad_up = jnp.einsum("rd,rf->df", entry_rows, dup, preferred_element_type=f32)
    dmerged = jnp.dot(late_resid, out_weight, preferred_element_type=f32)
    grad_gate_b = (dmerged * conv).astype(bf16)
    dconv = dmerged * gate_b.astype(f32)
    later = passed_along(dconv[:2], "sp", -1)
    extended_grad = jnp.concatenate([dconv, later], axis=0)
    dmixed = (
        taps[2] * extended_grad[:token_count]
        + taps[1] * extended_grad[1 : token_count + 1]
        + taps[0] * extended_grad[2 : token_count + 2]
    )
    grad_gate_c = (dmixed * values_u.astype(f32)).astype(bf16)
    grad_values = (dmixed * gate_c.astype(f32)).astype(bf16)
    return (
        grad_gate[None],
        grad_up[None],
        grad_down[None],
        grad_resid,
        grad_out_weight,
        grad_gate_b,
        grad_gate_c,
        grad_values,
    )


def solution(mesh):
    placed = (
        P("sp", None),
        P("sp", None),
        P(),
        P("sp", None),
        P("sp", None),
        P("sp", None, "tp"),
        P("sp", None, "tp"),
        P("sp", "tp", None),
        P(None, "tp"),
        P("sp", "tp"),
        P("sp", "tp"),
        P("sp", "tp"),
        P(None, "tp"),
    )

    return jax.shard_map(
        on_device,
        mesh=mesh,
        in_specs=placed,
        out_specs=(
            P("sp", None, "tp"),
            P("sp", None, "tp"),
            P("sp", "tp", None),
            P("sp", None),
            P("sp", "tp"),
            P("sp", "tp"),
            P("sp", "tp"),
            P("sp", "tp"),
        ),
        check_vma=False,
    )
```

```python
import jax
import jax.numpy as jnp
from jax import lax
from jax.experimental import pallas as pl
from jax.experimental.pallas import tpu as pltpu
from jax.sharding import PartitionSpec as P

norm_eps = 1e-06
direct_width = 128
f32 = jnp.float32
bf16 = jnp.bfloat16


def passed_along(array, axis, by):
    size = lax.axis_size(axis)
    pairs = [(i, i + by) for i in range(size) if 0 <= i + by < size]
    return lax.ppermute(array, axis, pairs)


def turned(array, by):
    size = lax.axis_size("tp")
    return lax.ppermute(array, "tp", [(i, (i + by) % size) for i in range(size)])


def exchanged(array):
    return lax.all_to_all(array, "sp", split_axis=0, concat_axis=0, tiled=True)


def ring_gather(piece):
    half = piece.shape[0] // 2
    prev = turned(piece, 1)
    nxt = turned(piece, -1)
    far_top = turned(prev[:half], 1)
    far_low = turned(nxt[half:], -1)
    return prev, nxt, far_top, far_low


def placed_columns(lane, pieces, width):
    piece, (prev, nxt, far_top, far_low) = pieces
    half = piece.shape[0] // 2
    size = piece.shape[1]
    lanes = width // size
    whole = jnp.zeros((piece.shape[0], width), piece.dtype)
    whole = lax.dynamic_update_slice(whole, piece, (0, lane * size))
    whole = lax.dynamic_update_slice(whole, prev, (0, ((lane + lanes - 1) % lanes) * size))
    whole = lax.dynamic_update_slice(whole, nxt, (0, ((lane + 1) % lanes) * size))
    far = ((lane + 2) % lanes) * size
    whole = lax.dynamic_update_slice(whole, far_top, (0, far))
    return lax.dynamic_update_slice(whole, far_low, (half, far))


def lane_gather(piece):
    others = []
    for way in (1, -1, 2):
        others.append(turned(piece, way))
    return piece, *others


lane_steps = (0, -1, 1, 2)


def finish_kernel(lane_ref, *refs):
    wide_refs, narrow_refs, direct_refs = refs[:4], refs[4:8], refs[8:12]
    cot_ref, resid_ref, gain_ref, out_ref, grad_ref = refs[12:]
    width = grad_ref.shape[1]
    quarter = width // 4
    wide = wide_refs[0].shape[1]
    for step, wide_ref, narrow_ref in zip(lane_steps, wide_refs, narrow_refs):
        start = ((lane_ref[0] + (4 + step)) % 4) * quarter
        grad_ref[:, pl.ds(pl.multiple_of(start, 128), wide)] = wide_ref[...].astype(f32)
        grad_ref[:, pl.ds(pl.multiple_of(start + wide, 128), direct_width)] = narrow_ref[
            ...
        ].astype(f32)
    direct = sum(ref[...].astype(f32) for ref in direct_refs)
    for place in range(4):
        end = (place + 1) * quarter
        grad_ref[:, end - direct_width : end] = direct[
            :, place * direct_width : (place + 1) * direct_width
        ]
    resid = resid_ref[...].astype(f32)
    inv_rms = lax.rsqrt(jnp.mean(resid * resid, axis=1, keepdims=True) + norm_eps)
    scaled = grad_ref[...] * gain_ref[...]
    inner = jnp.mean(scaled * resid, axis=1, keepdims=True)
    out_ref[...] = (
        cot_ref[...].astype(f32) + inv_rms * scaled - resid * (inv_rms**3 * inner)
    ).astype(bf16)


def finish(lane, pieces, cotangent, resid_in, norm_gain):
    tokens, width = cotangent.shape
    block = 128

    def rows(array):
        return pl.BlockSpec((block, array.shape[1]), lambda i, _: (i, 0))

    gain = norm_gain.reshape(1, width)
    return pl.pallas_call(
        finish_kernel,
        grid_spec=pltpu.PrefetchScalarGridSpec(
            num_scalar_prefetch=1,
            grid=(tokens // block,),
            in_specs=[rows(x) for x in (*pieces, cotangent, resid_in)]
            + [pl.BlockSpec((1, width), lambda i, _: (0, 0))],
            out_specs=pl.BlockSpec((block, width), lambda i, _: (i, 0)),
            scratch_shapes=[pltpu.VMEM((block, width), f32)],
        ),
        out_shape=jax.ShapeDtypeStruct((tokens, width), bf16),
    )(lane.reshape(1), *pieces, cotangent, resid_in, gain)


along_last = (((1,), (1,)), ((), ()))


def slot_pattern(block, at, count, capacity):
    slot = lax.broadcasted_iota(jnp.int32, (block, count), 0) + at
    low = lax.broadcasted_iota(jnp.int32, (block, count), 1) * capacity
    return ((slot >= low) & (slot < low + capacity)).astype(f32).astype(bf16)


def rows_kernel(lane_ref, routes_ref, share_ref, resid_ref, gain_ref, *refs):
    sent_ref, chooser_ref, rank_ref, high_ref, low_ref, normed_ref, turn_ref = refs
    tokens, quarter = normed_ref.shape
    experts = rank_ref.shape[1]
    block = chooser_ref.shape[0]
    capacity = 4 * tokens // experts
    step = pl.program_id(0)

    @pl.when(step == 0)
    def _():
        at = pl.ds(pl.multiple_of(lane_ref[0] * quarter, 128), quarter)
        some = 64

        def normalise(i, carry):
            rows = pl.ds(pl.multiple_of(i * some, some), some)
            wide = resid_ref[rows, :].astype(f32)
            inv_rms = lax.rsqrt(jnp.mean(wide * wide, axis=1, keepdims=True) + norm_eps)
            part = resid_ref[rows, at].astype(f32)
            normed_ref[rows, :] = (part * inv_rms * gain_ref[:, at]).astype(bf16)
            return carry

        lax.fori_loop(0, tokens // some, normalise, 0)
        ids = lax.broadcasted_iota(jnp.int32, (experts, tokens), 0)
        first = ids == routes_ref[0:1, :]
        second = ids == routes_ref[1:2, :]
        named = (first | second).astype(f32)
        share = jnp.where(first, share_ref[0:1, :], 0.0) + jnp.where(second, share_ref[1:2, :], 0.0)
        down = lax.broadcasted_iota(jnp.int32, (tokens, tokens), 0)
        over = lax.broadcasted_iota(jnp.int32, (tokens, tokens), 1)
        before = (down < over).astype(f32).astype(bf16)
        same = (over == down).astype(f32).astype(bf16)
        rank = jnp.dot(named.astype(bf16), before, preferred_element_type=f32)
        rank = jnp.where(named > 0.0, rank, -1.0).astype(bf16)
        turn_ref[...] = rank
        rank_ref[...] = lax.dot_general(
            same, rank, along_last, preferred_element_type=f32
        ).astype(bf16)
        high = share.astype(bf16)
        high_ref[...] = high
        low_ref[...] = (share - high.astype(f32)).astype(bf16)

    pattern = slot_pattern(block, step * block, experts, capacity)
    ranks = jnp.dot(pattern, turn_ref[...], preferred_element_type=f32)
    slot = lax.broadcasted_iota(jnp.int32, (block, 1), 0) + step * block
    wanted = lax.rem(slot, capacity).astype(f32)
    chooser = (ranks == wanted).astype(f32).astype(bf16)
    chooser_ref[...] = chooser
    sent_ref[...] = jnp.dot(chooser, normed_ref[...], preferred_element_type=f32).astype(bf16)


slot_block = 256


def chosen_rows(lane, routes, route_weights, resid_in, norm_gain, experts):
    tokens, width = resid_in.shape
    quarter = width // 4
    slots = 4 * tokens

    def whole(*shape):
        return pl.BlockSpec(shape, lambda i, _: (0, 0))

    return pl.pallas_call(
        rows_kernel,
        grid_spec=pltpu.PrefetchScalarGridSpec(
            num_scalar_prefetch=1,
            grid=(slots // slot_block,),
            in_specs=[whole(2, tokens), whole(2, tokens), whole(tokens, width), whole(1, width)],
            out_specs=[
                pl.BlockSpec((slot_block, quarter), lambda i, _: (i, 0)),
                pl.BlockSpec((slot_block, tokens), lambda i, _: (i, 0)),
                whole(tokens, experts),
                whole(experts, tokens),
                whole(experts, tokens),
            ],
            scratch_shapes=[pltpu.VMEM((tokens, quarter), bf16), pltpu.VMEM((experts, tokens), bf16)],
        ),
        out_shape=[
            jax.ShapeDtypeStruct((slots, quarter), bf16),
            jax.ShapeDtypeStruct((slots, tokens), bf16),
            jax.ShapeDtypeStruct((tokens, experts), bf16),
            jax.ShapeDtypeStruct((experts, tokens), bf16),
            jax.ShapeDtypeStruct((experts, tokens), bf16),
        ],
    )(lane.reshape(1), routes.T, route_weights.T, resid_in, norm_gain.reshape(1, width))


def weighted_kernel(chooser_ref, cot_ref, rank_ref, high_ref, low_ref, out_ref, token_ref):
    tokens, experts = rank_ref.shape
    block = chooser_ref.shape[0]
    capacity = 4 * tokens // experts
    at = pl.program_id(0) * block
    pattern = slot_pattern(block, at, experts, capacity)
    share = jnp.dot(pattern, high_ref[...], preferred_element_type=f32) + jnp.dot(
        pattern, low_ref[...], preferred_element_type=f32
    )
    chooser = chooser_ref[...]
    share = jnp.sum(share * chooser.astype(f32), axis=1, keepdims=True)
    width = out_ref.shape[1]
    part = 512
    for i in range(width // part):
        rows = jnp.dot(
            chooser, cot_ref[:, i * part : (i + 1) * part], preferred_element_type=f32
        )
        out_ref[:, i * part : (i + 1) * part] = (rows * share).astype(bf16)
    ranks = lax.dot_general(rank_ref[...], pattern, along_last, preferred_element_type=f32)
    slot = lax.broadcasted_iota(jnp.int32, (1, block), 1) + at
    token_ref[...] = (ranks == lax.rem(slot, capacity).astype(f32)).astype(f32).astype(bf16)


def weighted_rows(chooser, cotangent, rank, high, low):
    slots, tokens = chooser.shape
    width = cotangent.shape[1]

    def whole(array):
        return pl.BlockSpec(array.shape, lambda i: (0, 0))

    return pl.pallas_call(
        weighted_kernel,
        grid=(slots // slot_block,),
        in_specs=[pl.BlockSpec((slot_block, tokens), lambda i: (i, 0))]
        + [whole(x) for x in (cotangent, rank, high, low)],
        out_specs=[
            pl.BlockSpec((slot_block, width), lambda i: (i, 0)),
            pl.BlockSpec((tokens, slot_block), lambda i: (0, i)),
        ],
        out_shape=[
            jax.ShapeDtypeStruct((slots, width), bf16),
            jax.ShapeDtypeStruct((tokens, slots), bf16),
        ],
    )(chooser, cotangent, rank, high, low)


def expert_kernel(lane_ref, gate_ref, up_ref, cot_ref, down_ref, gmat_ref, umat_ref, *outs):
    hidden_ref, dgate_ref, dup_ref, direct_ref = outs[:4]
    further_refs = (outs[4:7], outs[7:10], outs[10:13], outs[13:16])
    quarter = gmat_ref.shape[0] // 4
    dhidden = lax.dot_general(
        cot_ref[...], down_ref[...], along_last, preferred_element_type=f32
    )
    gate_pre = gate_ref[...]
    up_pre = up_ref[...]
    logistic = jax.nn.sigmoid(gate_pre)
    activated = gate_pre * logistic
    hidden_ref[...] = (activated * up_pre).astype(bf16)
    dgate = (dhidden * up_pre * logistic * (1.0 + gate_pre * (1.0 - logistic))).astype(bf16)
    dup = (dhidden * activated).astype(bf16)
    dgate_ref[...] = dgate
    dup_ref[...] = dup
    for further in range(4):
        place = (lane_ref[0] + further) % 4
        at = pl.ds(pl.multiple_of(place * quarter, 128), quarter)
        part = lax.dot_general(
            dgate, gmat_ref[at, :], along_last, preferred_element_type=f32
        ) + lax.dot_general(dup, umat_ref[at, :], along_last, preferred_element_type=f32)
        part = part.astype(bf16)
        direct_ref[:, pl.ds(pl.multiple_of(place * direct_width, 128), direct_width)] = part[
            :, quarter - direct_width :
        ]
        for i, ref in enumerate(further_refs[further]):
            ref[...] = part[:, i * direct_width : (i + 1) * direct_width]


def expert_grads(lane, gate_pre, up_pre, entry_cots, down_mat, gate_mat, up_mat):
    slots, width = entry_cots.shape
    inner = gate_pre.shape[1]
    block = 256

    def rows(size):
        return pl.BlockSpec((block, size), lambda i, _: (i, 0))

    def whole(array):
        return pl.BlockSpec(array.shape, lambda i, _: (0, 0))

    sizes = [inner] * 3 + [4 * direct_width] + [direct_width] * 12
    return pl.pallas_call(
        expert_kernel,
        grid_spec=pltpu.PrefetchScalarGridSpec(
            num_scalar_prefetch=1,
            grid=(slots // block,),
            in_specs=[rows(inner), rows(inner), rows(width)]
            + [whole(x) for x in (down_mat, gate_mat, up_mat)],
            out_specs=[rows(size) for size in sizes],
        ),
        out_shape=[jax.ShapeDtypeStruct((slots, size), bf16) for size in sizes],
    )(lane.reshape(1), gate_pre, up_pre, entry_cots, down_mat, gate_mat, up_mat)


def on_device(
    resid_in,
    cotangent,
    norm_gain,
    routes,
    route_weights,
    gate_weight,
    up_weight,
    down_weight,
    out_weight,
    gate_b,
    gate_c,
    values_u,
    taps,
):
    token_count, model_width = resid_in.shape
    groups = lax.axis_size("sp")
    lanes = lax.axis_size("tp")
    lane = lax.axis_index("tp")
    expert_total = gate_weight.shape[0] * groups
    capacity = 4 * token_count // expert_total
    slots = expert_total * capacity
    quarter = model_width // lanes
    gate_mat, up_mat, down_mat = gate_weight[0], up_weight[0], down_weight[0]

    sent_rows, chooser, rank, high, low = chosen_rows(
        lane, routes, route_weights, resid_in, norm_gain, expert_total
    )
    got_part = exchanged(sent_rows.reshape(groups, capacity, quarter)).reshape(slots, quarter)
    sent_cots, token_chooser = weighted_rows(chooser, cotangent, rank, high, low)
    entry_cots = exchanged(sent_cots.reshape(groups, capacity, model_width))
    entry_cots = entry_cots.reshape(slots, model_width)
    entry_rows = placed_columns(lane, (got_part, ring_gather(got_part)), model_width)

    mixed = gate_c.astype(f32) * values_u.astype(f32)
    earlier = passed_along(mixed[-2:], "sp", 1)

    gate_pre = jnp.dot(entry_rows, gate_mat, preferred_element_type=f32)
    up_pre = jnp.dot(entry_rows, up_mat, preferred_element_type=f32)
    hidden, dgate, dup, direct, *others = expert_grads(
        lane, gate_pre, up_pre, entry_cots, down_mat, gate_mat, up_mat
    )
    a_own, b_own, c_own, a_ahead, b_ahead, c_ahead = others[:6]
    a_far, b_far, c_far, a_behind, b_behind, c_behind = others[6:]

    def back(array):
        return exchanged(array.reshape(groups, capacity, -1)).reshape(slots, -1)

    def per_token(array):
        return jnp.dot(token_chooser, array, preferred_element_type=f32).astype(bf16)

    def plus(*arrays):
        return sum(array.astype(f32) for array in arrays).astype(bf16)

    a_far = turned(a_far, 1)
    b_far = turned(b_far, -1)
    direct = back(direct)
    c_ahead, direct = lax.optimization_barrier((c_ahead, direct))
    a_next = turned(a_behind, -1)
    b_prev = turned(b_ahead, 1)
    a_prev = turned(plus(a_ahead, a_far), 1)
    b_next = turned(plus(b_behind, b_far), -1)
    c_far = turned(c_far, 1)
    c_next = turned(c_behind, -1)
    grad_down = jnp.einsum("rf,rd->fd", hidden, entry_cots, preferred_element_type=f32)
    wide = jnp.concatenate([plus(a_own, a_prev, a_next), plus(b_own, b_prev, b_next)], axis=1)
    c_own, wide = lax.optimization_barrier((c_own, wide))
    wide = back(wide)
    direct_parts = lane_gather(per_token(direct))
    c_prev = turned(plus(c_ahead, c_far), 1)
    narrow = back(plus(c_own, c_prev, c_next))
    wide_parts = lane_gather(per_token(wide))
    narrow_parts = lane_gather(per_token(narrow))
    pieces = (*wide_parts, *narrow_parts, *direct_parts)
    grad_resid = finish(lane, pieces, cotangent, resid_in, norm_gain)

    extended = jnp.concatenate([earlier, mixed], axis=0)
    conv = (
        taps[0] * extended[:token_count]
        + taps[1] * extended[1 : token_count + 1]
        + taps[2] * extended[2 : token_count + 2]
    )
    merged = (gate_b.astype(f32) * conv).astype(bf16)
    out_parts = jnp.einsum("td,tc->dc", grad_resid, merged, preferred_element_type=f32).astype(bf16)
    out_tiles = exchanged(out_parts.reshape(groups, model_width // groups, -1))
    grad_out_weight = jnp.sum(out_tiles.astype(f32), axis=0)
    dgate, out_parts = lax.optimization_barrier((dgate, out_parts))
    grad_gate = jnp.einsum("rd,rf->df", entry_rows, dgate, preferred_element_type=f32)
    late_resid, grad_gate, dup = lax.optimization_barrier((grad_resid, grad_gate, dup))
    grad_up = jnp.einsum("rd,rf->df", entry_rows, dup, preferred_element_type=f32)
    dmerged = jnp.dot(late_resid, out_weight, preferred_element_type=f32)
    grad_gate_b = (dmerged * conv).astype(bf16)
    dconv = dmerged * gate_b.astype(f32)
    later = passed_along(dconv[:2], "sp", -1)
    extended_grad = jnp.concatenate([dconv, later], axis=0)
    dmixed = (
        taps[2] * extended_grad[:token_count]
        + taps[1] * extended_grad[1 : token_count + 1]
        + taps[0] * extended_grad[2 : token_count + 2]
    )
    grad_gate_c = (dmixed * values_u.astype(f32)).astype(bf16)
    grad_values = (dmixed * gate_c.astype(f32)).astype(bf16)
    return (
        grad_gate[None],
        grad_up[None],
        grad_down[None],
        grad_resid,
        grad_out_weight,
        grad_gate_b,
        grad_gate_c,
        grad_values,
    )


def solution(mesh):
    placed = (
        P("sp", None),
        P("sp", None),
        P(),
        P("sp", None),
        P("sp", None),
        P("sp", None, "tp"),
        P("sp", None, "tp"),
        P("sp", "tp", None),
        P(None, "tp"),
        P("sp", "tp"),
        P("sp", "tp"),
        P("sp", "tp"),
        P(None, "tp"),
    )

    return jax.shard_map(
        on_device,
        mesh=mesh,
        in_specs=placed,
        out_specs=(
            P("sp", None, "tp"),
            P("sp", None, "tp"),
            P("sp", "tp", None),
            P("sp", None),
            P("sp", "tp"),
            P("sp", "tp"),
            P("sp", "tp"),
            P("sp", "tp"),
        ),
        check_vma=False,
    )
```

```python
import jax
import jax.numpy as jnp
from jax import lax
from jax.experimental import pallas as pl
from jax.experimental.pallas import tpu as pltpu
from jax.sharding import PartitionSpec as P

norm_eps = 1e-06
direct_width = 128
f32 = jnp.float32
bf16 = jnp.bfloat16


def passed_along(array, axis, by):
    size = lax.axis_size(axis)
    pairs = [(i, i + by) for i in range(size) if 0 <= i + by < size]
    return lax.ppermute(array, axis, pairs)


def turned(array, by):
    size = lax.axis_size("tp")
    return lax.ppermute(array, "tp", [(i, (i + by) % size) for i in range(size)])


def exchanged(array):
    return lax.all_to_all(array, "sp", split_axis=0, concat_axis=0, tiled=True)


def ring_gather(piece):
    half = piece.shape[0] // 2
    prev = turned(piece, 1)
    nxt = turned(piece, -1)
    far_top = turned(prev[:half], 1)
    far_low = turned(nxt[half:], -1)
    return prev, nxt, far_top, far_low


def place_kernel(lane_ref, own_ref, prev_ref, next_ref, top_ref, low_ref, out_ref):
    size = own_ref.shape[1]
    first_half = pl.program_id(0) < pl.num_programs(0) // 2

    def columns(further):
        return pl.ds(pl.multiple_of(((lane_ref[0] + further) % 4) * size, 128), size)

    out_ref[:, columns(0)] = own_ref[...]
    out_ref[:, columns(3)] = prev_ref[...]
    out_ref[:, columns(1)] = next_ref[...]

    @pl.when(first_half)
    def _():
        out_ref[:, columns(2)] = top_ref[...]

    @pl.when(jnp.logical_not(first_half))
    def _():
        out_ref[:, columns(2)] = low_ref[...]


def placed_columns(lane, piece, others):
    slots, size = piece.shape
    block = 192
    steps = slots // block
    half = steps // 2

    def rows(where):
        return pl.BlockSpec((block, size), lambda i, _: (where(i), 0))

    return pl.pallas_call(
        place_kernel,
        grid_spec=pltpu.PrefetchScalarGridSpec(
            num_scalar_prefetch=1,
            grid=(steps,),
            in_specs=[rows(lambda i: i)] * 3
            + [rows(lambda i: jnp.minimum(i, half - 1)), rows(lambda i: jnp.maximum(i - half, 0))],
            out_specs=pl.BlockSpec((block, 4 * size), lambda i, _: (i, 0)),
        ),
        out_shape=jax.ShapeDtypeStruct((slots, 4 * size), piece.dtype),
    )(lane.reshape(1), piece, *others)


def lane_gather(piece):
    others = []
    for way in (1, -1, 2):
        others.append(turned(piece, way))
    return piece, *others


lane_steps = (0, -1, 1, 2)


def finish_kernel(lane_ref, *refs):
    wide_refs, narrow_refs, direct_refs = refs[:4], refs[4:8], refs[8:12]
    cot_ref, resid_ref, gain_ref, out_ref, grad_ref = refs[12:]
    width = grad_ref.shape[1]
    quarter = width // 4
    wide = wide_refs[0].shape[1]
    some = grad_ref.shape[0]

    def some_rows(i, carry):
        rows = pl.ds(pl.multiple_of(i * some, some), some)
        for step, wide_ref, narrow_ref in zip(lane_steps, wide_refs, narrow_refs):
            start = ((lane_ref[0] + (4 + step)) % 4) * quarter
            grad_ref[:, pl.ds(pl.multiple_of(start, 128), wide)] = wide_ref[rows, :].astype(f32)
            grad_ref[:, pl.ds(pl.multiple_of(start + wide, 128), direct_width)] = narrow_ref[
                rows, :
            ].astype(f32)
        direct = sum(ref[rows, :].astype(f32) for ref in direct_refs)
        for place in range(4):
            end = (place + 1) * quarter
            grad_ref[:, end - direct_width : end] = direct[
                :, place * direct_width : (place + 1) * direct_width
            ]
        resid = resid_ref[rows, :].astype(f32)
        inv_rms = lax.rsqrt(jnp.mean(resid * resid, axis=1, keepdims=True) + norm_eps)
        scaled = grad_ref[...] * gain_ref[...]
        inner = jnp.mean(scaled * resid, axis=1, keepdims=True)
        out_ref[rows, :] = (
            cot_ref[rows, :].astype(f32) + inv_rms * scaled - resid * (inv_rms**3 * inner)
        ).astype(bf16)
        return carry

    lax.fori_loop(0, out_ref.shape[0] // some, some_rows, 0)


def finish(lane, pieces, cotangent, resid_in, norm_gain):
    tokens, width = cotangent.shape
    block = 192

    def rows(array):
        return pl.BlockSpec((block, array.shape[1]), lambda i, _: (i, 0))

    gain = norm_gain.reshape(1, width)
    return pl.pallas_call(
        finish_kernel,
        grid_spec=pltpu.PrefetchScalarGridSpec(
            num_scalar_prefetch=1,
            grid=(tokens // block,),
            in_specs=[rows(x) for x in (*pieces, cotangent, resid_in)]
            + [pl.BlockSpec((1, width), lambda i, _: (0, 0))],
            out_specs=pl.BlockSpec((block, width), lambda i, _: (i, 0)),
            scratch_shapes=[pltpu.VMEM((32, width), f32)],
        ),
        out_shape=jax.ShapeDtypeStruct((tokens, width), bf16),
    )(lane.reshape(1), *pieces, cotangent, resid_in, gain)


along_last = (((1,), (1,)), ((), ()))


def slot_pattern(block, at, count, capacity):
    slot = lax.broadcasted_iota(jnp.int32, (block, count), 0) + at
    low = lax.broadcasted_iota(jnp.int32, (block, count), 1) * capacity
    return ((slot >= low) & (slot < low + capacity)).astype(f32).astype(bf16)


def rows_kernel(lane_ref, routes_ref, share_ref, resid_ref, gain_ref, *refs):
    sent_ref, chooser_ref, rank_ref, high_ref, low_ref, normed_ref, turn_ref = refs
    tokens, quarter = normed_ref.shape
    experts = rank_ref.shape[1]
    block = chooser_ref.shape[0]
    capacity = 4 * tokens // experts
    step = pl.program_id(0)

    @pl.when(step == 0)
    def _():
        at = pl.ds(pl.multiple_of(lane_ref[0] * quarter, 128), quarter)
        some = 64

        def normalise(i, carry):
            rows = pl.ds(pl.multiple_of(i * some, some), some)
            wide = resid_ref[rows, :].astype(f32)
            inv_rms = lax.rsqrt(jnp.mean(wide * wide, axis=1, keepdims=True) + norm_eps)
            part = resid_ref[rows, at].astype(f32)
            normed_ref[rows, :] = (part * inv_rms * gain_ref[:, at]).astype(bf16)
            return carry

        lax.fori_loop(0, tokens // some, normalise, 0)
        ids = lax.broadcasted_iota(jnp.int32, (experts, tokens), 0)
        first = ids == routes_ref[0:1, :]
        second = ids == routes_ref[1:2, :]
        named = (first | second).astype(f32)
        share = jnp.where(first, share_ref[0:1, :], 0.0) + jnp.where(second, share_ref[1:2, :], 0.0)
        down = lax.broadcasted_iota(jnp.int32, (tokens, tokens), 0)
        over = lax.broadcasted_iota(jnp.int32, (tokens, tokens), 1)
        before = (down < over).astype(f32).astype(bf16)
        same = (over == down).astype(f32).astype(bf16)
        rank = jnp.dot(named.astype(bf16), before, preferred_element_type=f32)
        rank = jnp.where(named > 0.0, rank, -1.0).astype(bf16)
        turn_ref[...] = rank
        rank_ref[...] = lax.dot_general(
            same, rank, along_last, preferred_element_type=f32
        ).astype(bf16)
        high = share.astype(bf16)
        high_ref[...] = high
        low_ref[...] = (share - high.astype(f32)).astype(bf16)

    pattern = slot_pattern(block, step * block, experts, capacity)
    ranks = jnp.dot(pattern, turn_ref[...], preferred_element_type=f32)
    slot = lax.broadcasted_iota(jnp.int32, (block, 1), 0) + step * block
    wanted = lax.rem(slot, capacity).astype(f32)
    chooser = (ranks == wanted).astype(f32).astype(bf16)
    chooser_ref[...] = chooser
    sent_ref[...] = jnp.dot(chooser, normed_ref[...], preferred_element_type=f32).astype(bf16)


slot_block = 512


def chosen_rows(lane, routes, route_weights, resid_in, norm_gain, experts):
    tokens, width = resid_in.shape
    quarter = width // 4
    slots = 4 * tokens

    def whole(*shape):
        return pl.BlockSpec(shape, lambda i, _: (0, 0))

    return pl.pallas_call(
        rows_kernel,
        grid_spec=pltpu.PrefetchScalarGridSpec(
            num_scalar_prefetch=1,
            grid=(slots // slot_block,),
            in_specs=[whole(2, tokens), whole(2, tokens), whole(tokens, width), whole(1, width)],
            out_specs=[
                pl.BlockSpec((slot_block, quarter), lambda i, _: (i, 0)),
                pl.BlockSpec((slot_block, tokens), lambda i, _: (i, 0)),
                whole(tokens, experts),
                whole(experts, tokens),
                whole(experts, tokens),
            ],
            scratch_shapes=[pltpu.VMEM((tokens, quarter), bf16), pltpu.VMEM((experts, tokens), bf16)],
        ),
        out_shape=[
            jax.ShapeDtypeStruct((slots, quarter), bf16),
            jax.ShapeDtypeStruct((slots, tokens), bf16),
            jax.ShapeDtypeStruct((tokens, experts), bf16),
            jax.ShapeDtypeStruct((experts, tokens), bf16),
            jax.ShapeDtypeStruct((experts, tokens), bf16),
        ],
    )(lane.reshape(1), routes.T, route_weights.T, resid_in, norm_gain.reshape(1, width))


def weighted_kernel(chooser_ref, cot_ref, rank_ref, high_ref, low_ref, out_ref, token_ref):
    tokens, experts = rank_ref.shape
    block = chooser_ref.shape[0]
    capacity = 4 * tokens // experts
    at = pl.program_id(0) * block
    pattern = slot_pattern(block, at, experts, capacity)
    share = jnp.dot(pattern, high_ref[...], preferred_element_type=f32) + jnp.dot(
        pattern, low_ref[...], preferred_element_type=f32
    )
    chooser = chooser_ref[...]
    share = jnp.sum(share * chooser.astype(f32), axis=1, keepdims=True)
    width = out_ref.shape[1]
    part = 512

    def columns(i, carry):
        at = pl.ds(pl.multiple_of(i * part, part), part)
        rows = jnp.dot(chooser, cot_ref[:, at], preferred_element_type=f32)
        out_ref[:, at] = (rows * share).astype(bf16)
        return carry

    lax.fori_loop(0, width // part, columns, 0)
    ranks = lax.dot_general(rank_ref[...], pattern, along_last, preferred_element_type=f32)
    slot = lax.broadcasted_iota(jnp.int32, (1, block), 1) + at
    token_ref[...] = (ranks == lax.rem(slot, capacity).astype(f32)).astype(f32).astype(bf16)


def weighted_rows(chooser, cotangent, rank, high, low):
    slots, tokens = chooser.shape
    width = cotangent.shape[1]

    def whole(array):
        return pl.BlockSpec(array.shape, lambda i: (0, 0))

    return pl.pallas_call(
        weighted_kernel,
        grid=(slots // slot_block,),
        in_specs=[pl.BlockSpec((slot_block, tokens), lambda i: (i, 0))]
        + [whole(x) for x in (cotangent, rank, high, low)],
        out_specs=[
            pl.BlockSpec((slot_block, width), lambda i: (i, 0)),
            pl.BlockSpec((tokens, slot_block), lambda i: (0, i)),
        ],
        out_shape=[
            jax.ShapeDtypeStruct((slots, width), bf16),
            jax.ShapeDtypeStruct((tokens, slots), bf16),
        ],
    )(chooser, cotangent, rank, high, low)


def on_device(
    resid_in,
    cotangent,
    norm_gain,
    routes,
    route_weights,
    gate_weight,
    up_weight,
    down_weight,
    out_weight,
    gate_b,
    gate_c,
    values_u,
    taps,
):
    token_count, model_width = resid_in.shape
    groups = lax.axis_size("sp")
    lanes = lax.axis_size("tp")
    lane = lax.axis_index("tp")
    expert_total = gate_weight.shape[0] * groups
    capacity = 4 * token_count // expert_total
    slots = expert_total * capacity
    quarter = model_width // lanes
    gate_mat, up_mat, down_mat = gate_weight[0], up_weight[0], down_weight[0]

    sent_rows, chooser, rank, high, low = chosen_rows(
        lane, routes, route_weights, resid_in, norm_gain, expert_total
    )
    got_part = exchanged(sent_rows.reshape(groups, capacity, quarter)).reshape(slots, quarter)
    sent_cots, token_chooser = weighted_rows(chooser, cotangent, rank, high, low)
    entry_cots = exchanged(sent_cots.reshape(groups, capacity, model_width))
    entry_cots = entry_cots.reshape(slots, model_width)
    entry_rows = placed_columns(lane, got_part, ring_gather(got_part))

    mixed = gate_c.astype(f32) * values_u.astype(f32)
    earlier = passed_along(mixed[-2:], "sp", 1)

    both_mat = jnp.concatenate([gate_mat, up_mat], axis=1)
    direct_mat = both_mat.reshape(lanes, quarter, -1)[:, -direct_width:].reshape(
        lanes * direct_width, -1
    )
    both_mat, direct_mat = lax.optimization_barrier((both_mat, direct_mat))
    gate_pre = jnp.dot(entry_rows, gate_mat, preferred_element_type=f32)
    up_pre = jnp.dot(entry_rows, up_mat, preferred_element_type=f32)
    logistic = jax.nn.sigmoid(gate_pre)
    activated = gate_pre * logistic
    hidden = (activated * up_pre).astype(bf16)
    slope = up_pre * logistic * (1.0 + gate_pre * (1.0 - logistic))
    activated, slope, hidden = lax.optimization_barrier((activated, slope, hidden))
    dhidden = jnp.einsum("rd,fd->rf", entry_cots, down_mat, preferred_element_type=f32)
    dgate = (dhidden * slope).astype(bf16)
    dup = (dhidden * activated).astype(bf16)
    dboth = jnp.concatenate([dgate, dup], axis=1)

    def back(array):
        return exchanged(array.reshape(groups, capacity, -1)).reshape(slots, -1)

    def per_token(array):
        return jnp.dot(token_chooser, array, preferred_element_type=f32).astype(bf16)

    def plus(*arrays):
        return sum(array.astype(f32) for array in arrays).astype(bf16)

    def part(further, first, count, rows=slice(None)):
        at = ((lane + further) % lanes) * quarter + first * direct_width
        mat = lax.dynamic_slice_in_dim(both_mat, at, count * direct_width, axis=0)
        return jnp.einsum("rf,df->rd", dboth[rows], mat, preferred_element_type=f32)

    top, low = slice(None, slots // 2), slice(slots // 2, None)
    a_far = turned(part(2, 0, 2, top).astype(bf16), 1)
    b_far = turned(part(2, 0, 2, low).astype(bf16), -1)
    direct = jnp.einsum("rf,df->rd", dboth, direct_mat, preferred_element_type=f32)
    direct = back(direct.astype(bf16))
    a_next = turned(part(3, 0, 2, top).astype(bf16), -1)
    b_prev = turned(part(1, 0, 2, low).astype(bf16), 1)
    a_prev = turned((part(1, 0, 2, top) + a_far.astype(f32)).astype(bf16), 1)
    b_next = turned((part(3, 0, 2, low) + b_far.astype(f32)).astype(bf16), -1)
    c_far, c_behind, own, c_own, c_ahead = (
        part(*which).astype(bf16)
        for which in ((2, 2, 1), (3, 2, 1), (0, 0, 2), (0, 2, 1), (1, 2, 1))
    )
    c_far = turned(c_far, 1)
    c_next = turned(c_behind, -1)
    c_ahead, direct = lax.optimization_barrier((c_ahead, direct))
    grad_down = jnp.einsum("rf,rd->fd", hidden, entry_cots, preferred_element_type=f32)
    wide = plus(
        own,
        jnp.concatenate([a_prev, b_prev], axis=0),
        jnp.concatenate([a_next, b_next], axis=0),
    )
    c_own, wide = lax.optimization_barrier((c_own, wide))
    wide = back(wide)
    direct_parts = lane_gather(per_token(direct))
    c_prev = turned(plus(c_ahead, c_far), 1)
    narrow = back(plus(c_own, c_prev, c_next))
    wide_parts = lane_gather(per_token(wide))
    narrow_parts = lane_gather(per_token(narrow))
    pieces = (*wide_parts, *narrow_parts, *direct_parts)
    grad_resid = finish(lane, pieces, cotangent, resid_in, norm_gain)

    extended = jnp.concatenate([earlier, mixed], axis=0)
    conv = (
        taps[0] * extended[:token_count]
        + taps[1] * extended[1 : token_count + 1]
        + taps[2] * extended[2 : token_count + 2]
    )
    merged = (gate_b.astype(f32) * conv).astype(bf16)
    out_parts = jnp.einsum("td,tc->dc", grad_resid, merged, preferred_element_type=f32).astype(bf16)
    out_tiles = exchanged(out_parts.reshape(groups, model_width // groups, -1))
    grad_out_weight = jnp.sum(out_tiles.astype(f32), axis=0)
    late_both, out_parts = lax.optimization_barrier((dboth, out_parts))
    grad_both = jnp.einsum("rd,rf->df", entry_rows, late_both, preferred_element_type=f32)
    late_resid, grad_both = lax.optimization_barrier((grad_resid, grad_both))
    grad_gate, grad_up = jnp.split(grad_both, 2, axis=1)
    dmerged = jnp.dot(late_resid, out_weight, preferred_element_type=f32)
    grad_gate_b = (dmerged * conv).astype(bf16)
    dconv = dmerged * gate_b.astype(f32)
    later = passed_along(dconv[:2], "sp", -1)
    extended_grad = jnp.concatenate([dconv, later], axis=0)
    dmixed = (
        taps[2] * extended_grad[:token_count]
        + taps[1] * extended_grad[1 : token_count + 1]
        + taps[0] * extended_grad[2 : token_count + 2]
    )
    grad_gate_c = (dmixed * values_u.astype(f32)).astype(bf16)
    grad_values = (dmixed * gate_c.astype(f32)).astype(bf16)
    return (
        grad_gate[None],
        grad_up[None],
        grad_down[None],
        grad_resid,
        grad_out_weight,
        grad_gate_b,
        grad_gate_c,
        grad_values,
    )


def solution(mesh):
    placed = (
        P("sp", None),
        P("sp", None),
        P(),
        P("sp", None),
        P("sp", None),
        P("sp", None, "tp"),
        P("sp", None, "tp"),
        P("sp", "tp", None),
        P(None, "tp"),
        P("sp", "tp"),
        P("sp", "tp"),
        P("sp", "tp"),
        P(None, "tp"),
    )

    return jax.shard_map(
        on_device,
        mesh=mesh,
        in_specs=placed,
        out_specs=(
            P("sp", None, "tp"),
            P("sp", None, "tp"),
            P("sp", "tp", None),
            P("sp", None),
            P("sp", "tp"),
            P("sp", "tp"),
            P("sp", "tp"),
            P("sp", "tp"),
        ),
        check_vma=False,
    )
```

```python
import jax
import jax.numpy as jnp
from jax import lax
from jax.experimental import pallas as pl
from jax.experimental.pallas import tpu as pltpu
from jax.sharding import PartitionSpec as P

norm_eps = 1e-06
direct_width = 128
f32 = jnp.float32
bf16 = jnp.bfloat16


def passed_along(array, axis, by):
    size = lax.axis_size(axis)
    pairs = [(i, i + by) for i in range(size) if 0 <= i + by < size]
    return lax.ppermute(array, axis, pairs)


def turned(array, by):
    size = lax.axis_size("tp")
    return lax.ppermute(array, "tp", [(i, (i + by) % size) for i in range(size)])


def exchanged(array):
    return lax.all_to_all(array, "sp", split_axis=0, concat_axis=0, tiled=True)


def ring_gather(piece):
    half = piece.shape[0] // 2
    prev = turned(piece, 1)
    nxt = turned(piece, -1)
    far_top = turned(prev[:half], 1)
    far_low = turned(nxt[half:], -1)
    return prev, nxt, far_top, far_low


def placed_columns(lane, pieces, width):
    piece, (prev, nxt, far_top, far_low) = pieces
    half = piece.shape[0] // 2
    size = piece.shape[1]
    lanes = width // size
    whole = jnp.zeros((piece.shape[0], width), piece.dtype)
    whole = lax.dynamic_update_slice(whole, piece, (0, lane * size))
    whole = lax.dynamic_update_slice(whole, prev, (0, ((lane + lanes - 1) % lanes) * size))
    whole = lax.dynamic_update_slice(whole, nxt, (0, ((lane + 1) % lanes) * size))
    far = ((lane + 2) % lanes) * size
    whole = lax.dynamic_update_slice(whole, far_top, (0, far))
    return lax.dynamic_update_slice(whole, far_low, (half, far))


def lane_gather(piece):
    others = []
    for way in (1, -1, 2):
        others.append(turned(piece, way))
    return piece, *others


lane_steps = (0, -1, 1, 2)


def finish_kernel(lane_ref, *refs):
    wide_refs, narrow_refs, direct_refs = refs[:4], refs[4:8], refs[8:12]
    cot_ref, resid_ref, gain_ref, out_ref, grad_ref = refs[12:]
    width = grad_ref.shape[1]
    quarter = width // 4
    wide = wide_refs[0].shape[1]
    for step, wide_ref, narrow_ref in zip(lane_steps, wide_refs, narrow_refs):
        start = ((lane_ref[0] + (4 + step)) % 4) * quarter
        grad_ref[:, pl.ds(pl.multiple_of(start, 128), wide)] = wide_ref[...].astype(f32)
        grad_ref[:, pl.ds(pl.multiple_of(start + wide, 128), direct_width)] = narrow_ref[
            ...
        ].astype(f32)
    direct = sum(ref[...].astype(f32) for ref in direct_refs)
    for place in range(4):
        end = (place + 1) * quarter
        grad_ref[:, end - direct_width : end] = direct[
            :, place * direct_width : (place + 1) * direct_width
        ]
    resid = resid_ref[...].astype(f32)
    inv_rms = lax.rsqrt(jnp.mean(resid * resid, axis=1, keepdims=True) + norm_eps)
    scaled = grad_ref[...] * gain_ref[...]
    inner = jnp.mean(scaled * resid, axis=1, keepdims=True)
    out_ref[...] = (
        cot_ref[...].astype(f32) + inv_rms * scaled - resid * (inv_rms**3 * inner)
    ).astype(bf16)


def finish(lane, pieces, cotangent, resid_in, norm_gain):
    tokens, width = cotangent.shape
    block = 192

    def rows(array):
        return pl.BlockSpec((block, array.shape[1]), lambda i, _: (i, 0))

    gain = norm_gain.reshape(1, width)
    return pl.pallas_call(
        finish_kernel,
        grid_spec=pltpu.PrefetchScalarGridSpec(
            num_scalar_prefetch=1,
            grid=(tokens // block,),
            in_specs=[rows(x) for x in (*pieces, cotangent, resid_in)]
            + [pl.BlockSpec((1, width), lambda i, _: (0, 0))],
            out_specs=pl.BlockSpec((block, width), lambda i, _: (i, 0)),
            scratch_shapes=[pltpu.VMEM((block, width), f32)],
        ),
        out_shape=jax.ShapeDtypeStruct((tokens, width), bf16),
    )(lane.reshape(1), *pieces, cotangent, resid_in, gain)


along_last = (((1,), (1,)), ((), ()))


def slot_pattern(block, at, count, capacity):
    slot = lax.broadcasted_iota(jnp.int32, (block, count), 0) + at
    low = lax.broadcasted_iota(jnp.int32, (block, count), 1) * capacity
    return ((slot >= low) & (slot < low + capacity)).astype(f32).astype(bf16)


def rows_kernel(lane_ref, routes_ref, share_ref, resid_ref, gain_ref, *refs):
    sent_ref, chooser_ref, rank_ref, high_ref, low_ref, normed_ref, turn_ref = refs
    tokens, quarter = normed_ref.shape
    experts = rank_ref.shape[1]
    block = chooser_ref.shape[0]
    capacity = 4 * tokens // experts
    step = pl.program_id(0)

    @pl.when(step == 0)
    def _():
        at = pl.ds(pl.multiple_of(lane_ref[0] * quarter, 128), quarter)
        some = 64

        def normalise(i, carry):
            rows = pl.ds(pl.multiple_of(i * some, some), some)
            wide = resid_ref[rows, :].astype(f32)
            inv_rms = lax.rsqrt(jnp.mean(wide * wide, axis=1, keepdims=True) + norm_eps)
            part = resid_ref[rows, at].astype(f32)
            normed_ref[rows, :] = (part * inv_rms * gain_ref[:, at]).astype(bf16)
            return carry

        lax.fori_loop(0, tokens // some, normalise, 0)
        ids = lax.broadcasted_iota(jnp.int32, (experts, tokens), 0)
        first = ids == routes_ref[0:1, :]
        second = ids == routes_ref[1:2, :]
        named = (first | second).astype(f32)
        share = jnp.where(first, share_ref[0:1, :], 0.0) + jnp.where(second, share_ref[1:2, :], 0.0)
        down = lax.broadcasted_iota(jnp.int32, (tokens, tokens), 0)
        over = lax.broadcasted_iota(jnp.int32, (tokens, tokens), 1)
        before = (down < over).astype(f32).astype(bf16)
        same = (over == down).astype(f32).astype(bf16)
        rank = jnp.dot(named.astype(bf16), before, preferred_element_type=f32)
        rank = jnp.where(named > 0.0, rank, -1.0).astype(bf16)
        turn_ref[...] = rank
        rank_ref[...] = lax.dot_general(
            same, rank, along_last, preferred_element_type=f32
        ).astype(bf16)
        high = share.astype(bf16)
        high_ref[...] = high
        low_ref[...] = (share - high.astype(f32)).astype(bf16)

    pattern = slot_pattern(block, step * block, experts, capacity)
    ranks = jnp.dot(pattern, turn_ref[...], preferred_element_type=f32)
    slot = lax.broadcasted_iota(jnp.int32, (block, 1), 0) + step * block
    wanted = lax.rem(slot, capacity).astype(f32)
    chooser = (ranks == wanted).astype(f32).astype(bf16)
    chooser_ref[...] = chooser
    sent_ref[...] = jnp.dot(chooser, normed_ref[...], preferred_element_type=f32).astype(bf16)


slot_block = 512


def chosen_rows(lane, routes, route_weights, resid_in, norm_gain, experts):
    tokens, width = resid_in.shape
    quarter = width // 4
    slots = 4 * tokens

    def whole(*shape):
        return pl.BlockSpec(shape, lambda i, _: (0, 0))

    return pl.pallas_call(
        rows_kernel,
        grid_spec=pltpu.PrefetchScalarGridSpec(
            num_scalar_prefetch=1,
            grid=(slots // slot_block,),
            in_specs=[whole(2, tokens), whole(2, tokens), whole(tokens, width), whole(1, width)],
            out_specs=[
                pl.BlockSpec((slot_block, quarter), lambda i, _: (i, 0)),
                pl.BlockSpec((slot_block, tokens), lambda i, _: (i, 0)),
                whole(tokens, experts),
                whole(experts, tokens),
                whole(experts, tokens),
            ],
            scratch_shapes=[pltpu.VMEM((tokens, quarter), bf16), pltpu.VMEM((experts, tokens), bf16)],
        ),
        out_shape=[
            jax.ShapeDtypeStruct((slots, quarter), bf16),
            jax.ShapeDtypeStruct((slots, tokens), bf16),
            jax.ShapeDtypeStruct((tokens, experts), bf16),
            jax.ShapeDtypeStruct((experts, tokens), bf16),
            jax.ShapeDtypeStruct((experts, tokens), bf16),
        ],
    )(lane.reshape(1), routes.T, route_weights.T, resid_in, norm_gain.reshape(1, width))


def weighted_kernel(chooser_ref, cot_ref, rank_ref, high_ref, low_ref, out_ref, token_ref):
    tokens, experts = rank_ref.shape
    block = chooser_ref.shape[0]
    capacity = 4 * tokens // experts
    at = pl.program_id(0) * block
    pattern = slot_pattern(block, at, experts, capacity)
    share = jnp.dot(pattern, high_ref[...], preferred_element_type=f32) + jnp.dot(
        pattern, low_ref[...], preferred_element_type=f32
    )
    chooser = chooser_ref[...]
    share = jnp.sum(share * chooser.astype(f32), axis=1, keepdims=True)
    width = out_ref.shape[1]
    part = 512
    for i in range(width // part):
        rows = jnp.dot(
            chooser, cot_ref[:, i * part : (i + 1) * part], preferred_element_type=f32
        )
        out_ref[:, i * part : (i + 1) * part] = (rows * share).astype(bf16)
    ranks = lax.dot_general(rank_ref[...], pattern, along_last, preferred_element_type=f32)
    slot = lax.broadcasted_iota(jnp.int32, (1, block), 1) + at
    token_ref[...] = (ranks == lax.rem(slot, capacity).astype(f32)).astype(f32).astype(bf16)


def weighted_rows(chooser, cotangent, rank, high, low):
    slots, tokens = chooser.shape
    width = cotangent.shape[1]

    def whole(array):
        return pl.BlockSpec(array.shape, lambda i: (0, 0))

    return pl.pallas_call(
        weighted_kernel,
        grid=(slots // slot_block,),
        in_specs=[pl.BlockSpec((slot_block, tokens), lambda i: (i, 0))]
        + [whole(x) for x in (cotangent, rank, high, low)],
        out_specs=[
            pl.BlockSpec((slot_block, width), lambda i: (i, 0)),
            pl.BlockSpec((tokens, slot_block), lambda i: (0, i)),
        ],
        out_shape=[
            jax.ShapeDtypeStruct((slots, width), bf16),
            jax.ShapeDtypeStruct((tokens, slots), bf16),
        ],
    )(chooser, cotangent, rank, high, low)


def write_parts(both, mat_ref, refs):
    part = lax.dot_general(both, mat_ref[...], along_last, preferred_element_type=f32)
    part = part.astype(bf16)
    at = 0
    for ref in refs:
        ref[...] = part[:, at : at + ref.shape[1]]
        at += ref.shape[1]


def first_kernel(cot_ref, act_ref, slope_ref, down_ref, mat_ref, both_ref, *refs):
    dhidden = lax.dot_general(
        cot_ref[...], down_ref[...], along_last, preferred_element_type=f32
    )
    dgate = (dhidden * slope_ref[...].astype(f32)).astype(bf16)
    dup = (dhidden * act_ref[...].astype(f32)).astype(bf16)
    both = jnp.concatenate([dgate, dup], axis=1)
    both_ref[...] = both
    write_parts(both, mat_ref, refs)


def other_kernel(both_ref, mat_ref, *refs):
    write_parts(both_ref[...], mat_ref, refs)


part_block = 512


def by_rows(kernel, rowwise, matrices, sizes):
    slots = rowwise[0].shape[0]

    def rows(size):
        return pl.BlockSpec((part_block, size), lambda i: (i, 0))

    return pl.pallas_call(
        kernel,
        grid=(slots // part_block,),
        in_specs=[rows(x.shape[1]) for x in rowwise]
        + [pl.BlockSpec(x.shape, lambda i: (0, 0)) for x in matrices],
        out_specs=[rows(size) for size in sizes],
        out_shape=[jax.ShapeDtypeStruct((slots, size), bf16) for size in sizes],
    )(*rowwise, *matrices)


def on_device(
    resid_in,
    cotangent,
    norm_gain,
    routes,
    route_weights,
    gate_weight,
    up_weight,
    down_weight,
    out_weight,
    gate_b,
    gate_c,
    values_u,
    taps,
):
    token_count, model_width = resid_in.shape
    groups = lax.axis_size("sp")
    lanes = lax.axis_size("tp")
    lane = lax.axis_index("tp")
    expert_total = gate_weight.shape[0] * groups
    capacity = 4 * token_count // expert_total
    slots = expert_total * capacity
    quarter = model_width // lanes
    gate_mat, up_mat, down_mat = gate_weight[0], up_weight[0], down_weight[0]

    sent_rows, chooser, rank, high, low = chosen_rows(
        lane, routes, route_weights, resid_in, norm_gain, expert_total
    )
    got_part = exchanged(sent_rows.reshape(groups, capacity, quarter)).reshape(slots, quarter)
    sent_cots, token_chooser = weighted_rows(chooser, cotangent, rank, high, low)
    entry_cots = exchanged(sent_cots.reshape(groups, capacity, model_width))
    entry_cots = entry_cots.reshape(slots, model_width)
    entry_rows = placed_columns(lane, (got_part, ring_gather(got_part)), model_width)

    mixed = gate_c.astype(f32) * values_u.astype(f32)
    earlier = passed_along(mixed[-2:], "sp", 1)

    gate_pre = jnp.dot(entry_rows, gate_mat, preferred_element_type=f32)
    up_pre = jnp.dot(entry_rows, up_mat, preferred_element_type=f32)
    logistic = jax.nn.sigmoid(gate_pre)
    activated = gate_pre * logistic
    hidden = (activated * up_pre).astype(bf16)
    slope = up_pre * logistic * (1.0 + gate_pre * (1.0 - logistic))
    both_mat = jnp.concatenate([gate_mat, up_mat], axis=1)

    def weight_rows(further, first, count):
        at = ((lane + further) % lanes) * quarter + first * direct_width
        return lax.dynamic_slice_in_dim(both_mat, at, count * direct_width, axis=0)

    direct_mat = both_mat.reshape(lanes, quarter, -1)[:, -direct_width:]
    first_mat = jnp.concatenate(
        [weight_rows(2, 0, 2), weight_rows(3, 0, 1), weight_rows(1, 1, 1)]
        + [direct_mat.reshape(lanes * direct_width, -1)],
        axis=0,
    )
    other_mat = jnp.concatenate(
        [weight_rows(0, 0, 3), weight_rows(1, 0, 1), weight_rows(1, 2, 1)]
        + [weight_rows(3, 1, 2), weight_rows(2, 2, 1)],
        axis=0,
    )
    activated, slope, hidden, first_mat, other_mat = lax.optimization_barrier(
        (activated.astype(bf16), slope.astype(bf16), hidden, first_mat, other_mat)
    )
    dboth, a_far, b_far, a_behind, b_ahead, direct = by_rows(
        first_kernel,
        (entry_cots, activated, slope),
        (down_mat, first_mat),
        [both_mat.shape[1]] + [direct_width] * 4 + [lanes * direct_width],
    )
    a_own, b_own, c_own, a_ahead, c_ahead, b_behind, c_behind, c_far = by_rows(
        other_kernel, (dboth,), (other_mat,), [direct_width] * 8
    )

    def back(array):
        return exchanged(array.reshape(groups, capacity, -1)).reshape(slots, -1)

    def per_token(array):
        return jnp.dot(token_chooser, array, preferred_element_type=f32).astype(bf16)

    def plus(*arrays):
        return sum(array.astype(f32) for array in arrays).astype(bf16)

    a_far = turned(a_far, 1)
    b_far = turned(b_far, -1)
    direct = back(direct)
    c_ahead, direct = lax.optimization_barrier((c_ahead, direct))
    a_next = turned(a_behind, -1)
    b_prev = turned(b_ahead, 1)
    a_prev = turned(plus(a_ahead, a_far), 1)
    b_next = turned(plus(b_behind, b_far), -1)
    c_far = turned(c_far, 1)
    c_next = turned(c_behind, -1)
    grad_down = jnp.einsum("rf,rd->fd", hidden, entry_cots, preferred_element_type=f32)
    wide = jnp.concatenate([plus(a_own, a_prev, a_next), plus(b_own, b_prev, b_next)], axis=1)
    c_own, wide = lax.optimization_barrier((c_own, wide))
    wide = back(wide)
    direct_parts = lane_gather(per_token(direct))
    c_prev = turned(plus(c_ahead, c_far), 1)
    narrow = back(plus(c_own, c_prev, c_next))
    wide_parts = lane_gather(per_token(wide))
    narrow_parts = lane_gather(per_token(narrow))
    pieces = (*wide_parts, *narrow_parts, *direct_parts)
    grad_resid = finish(lane, pieces, cotangent, resid_in, norm_gain)

    extended = jnp.concatenate([earlier, mixed], axis=0)
    conv = (
        taps[0] * extended[:token_count]
        + taps[1] * extended[1 : token_count + 1]
        + taps[2] * extended[2 : token_count + 2]
    )
    merged = (gate_b.astype(f32) * conv).astype(bf16)
    out_parts = jnp.einsum("td,tc->dc", grad_resid, merged, preferred_element_type=f32).astype(bf16)
    out_tiles = exchanged(out_parts.reshape(groups, model_width // groups, -1))
    grad_out_weight = jnp.sum(out_tiles.astype(f32), axis=0)
    late_both, out_parts = lax.optimization_barrier((dboth, out_parts))
    grad_both = jnp.einsum("rd,rf->df", entry_rows, late_both, preferred_element_type=f32)
    late_resid, grad_both = lax.optimization_barrier((grad_resid, grad_both))
    grad_gate, grad_up = jnp.split(grad_both, 2, axis=1)
    dmerged = jnp.dot(late_resid, out_weight, preferred_element_type=f32)
    grad_gate_b = (dmerged * conv).astype(bf16)
    dconv = dmerged * gate_b.astype(f32)
    later = passed_along(dconv[:2], "sp", -1)
    extended_grad = jnp.concatenate([dconv, later], axis=0)
    dmixed = (
        taps[2] * extended_grad[:token_count]
        + taps[1] * extended_grad[1 : token_count + 1]
        + taps[0] * extended_grad[2 : token_count + 2]
    )
    grad_gate_c = (dmixed * values_u.astype(f32)).astype(bf16)
    grad_values = (dmixed * gate_c.astype(f32)).astype(bf16)
    return (
        grad_gate[None],
        grad_up[None],
        grad_down[None],
        grad_resid,
        grad_out_weight,
        grad_gate_b,
        grad_gate_c,
        grad_values,
    )


def solution(mesh):
    placed = (
        P("sp", None),
        P("sp", None),
        P(),
        P("sp", None),
        P("sp", None),
        P("sp", None, "tp"),
        P("sp", None, "tp"),
        P("sp", "tp", None),
        P(None, "tp"),
        P("sp", "tp"),
        P("sp", "tp"),
        P("sp", "tp"),
        P(None, "tp"),
    )

    return jax.shard_map(
        on_device,
        mesh=mesh,
        in_specs=placed,
        out_specs=(
            P("sp", None, "tp"),
            P("sp", None, "tp"),
            P("sp", "tp", None),
            P("sp", None),
            P("sp", "tp"),
            P("sp", "tp"),
            P("sp", "tp"),
            P("sp", "tp"),
        ),
        check_vma=False,
    )
```

```python
import jax
import jax.numpy as jnp
from jax import lax
from jax.experimental import pallas as pl
from jax.experimental.pallas import tpu as pltpu
from jax.sharding import PartitionSpec as P

norm_eps = 1e-06
direct_width = 128
f32 = jnp.float32
bf16 = jnp.bfloat16


def passed_along(array, axis, by):
    size = lax.axis_size(axis)
    pairs = [(i, i + by) for i in range(size) if 0 <= i + by < size]
    return lax.ppermute(array, axis, pairs)


def turned(array, by):
    size = lax.axis_size("tp")
    return lax.ppermute(array, "tp", [(i, (i + by) % size) for i in range(size)])


def exchanged(array):
    return lax.all_to_all(array, "sp", split_axis=0, concat_axis=0, tiled=True)


def ring_gather(piece):
    half = piece.shape[0] // 2
    prev = turned(piece, 1)
    nxt = turned(piece, -1)
    far_top = turned(prev[:half], 1)
    far_low = turned(nxt[half:], -1)
    return prev, nxt, far_top, far_low


def placed_columns(lane, pieces, width):
    piece, (prev, nxt, far_top, far_low) = pieces
    half = piece.shape[0] // 2
    size = piece.shape[1]
    lanes = width // size
    whole = jnp.zeros((piece.shape[0], width), piece.dtype)
    whole = lax.dynamic_update_slice(whole, piece, (0, lane * size))
    whole = lax.dynamic_update_slice(whole, prev, (0, ((lane + lanes - 1) % lanes) * size))
    whole = lax.dynamic_update_slice(whole, nxt, (0, ((lane + 1) % lanes) * size))
    far = ((lane + 2) % lanes) * size
    whole = lax.dynamic_update_slice(whole, far_top, (0, far))
    return lax.dynamic_update_slice(whole, far_low, (half, far))


def lane_gather(piece):
    others = []
    for way in (1, -1, 2):
        others.append(turned(piece, way))
    return piece, *others


lane_steps = (0, -1, 1, 2)


def finish_kernel(lane_ref, *refs):
    wide_refs, narrow_refs, direct_refs = refs[:4], refs[4:8], refs[8:12]
    cot_ref, resid_ref, gain_ref, out_ref, grad_ref = refs[12:]
    width = grad_ref.shape[1]
    quarter = width // 4
    wide = wide_refs[0].shape[1]
    for step, wide_ref, narrow_ref in zip(lane_steps, wide_refs, narrow_refs):
        start = ((lane_ref[0] + (4 + step)) % 4) * quarter
        grad_ref[:, pl.ds(pl.multiple_of(start, 128), wide)] = wide_ref[...].astype(f32)
        grad_ref[:, pl.ds(pl.multiple_of(start + wide, 128), direct_width)] = narrow_ref[
            ...
        ].astype(f32)
    direct = sum(ref[...].astype(f32) for ref in direct_refs)
    for place in range(4):
        end = (place + 1) * quarter
        grad_ref[:, end - direct_width : end] = direct[
            :, place * direct_width : (place + 1) * direct_width
        ]
    resid = resid_ref[...].astype(f32)
    inv_rms = lax.rsqrt(jnp.mean(resid * resid, axis=1, keepdims=True) + norm_eps)
    scaled = grad_ref[...] * gain_ref[...]
    inner = jnp.mean(scaled * resid, axis=1, keepdims=True)
    out_ref[...] = (
        cot_ref[...].astype(f32) + inv_rms * scaled - resid * (inv_rms**3 * inner)
    ).astype(bf16)


def finish(lane, pieces, cotangent, resid_in, norm_gain):
    tokens, width = cotangent.shape
    block = 192

    def rows(array):
        return pl.BlockSpec((block, array.shape[1]), lambda i, _: (i, 0))

    gain = norm_gain.reshape(1, width)
    return pl.pallas_call(
        finish_kernel,
        grid_spec=pltpu.PrefetchScalarGridSpec(
            num_scalar_prefetch=1,
            grid=(tokens // block,),
            in_specs=[rows(x) for x in (*pieces, cotangent, resid_in)]
            + [pl.BlockSpec((1, width), lambda i, _: (0, 0))],
            out_specs=pl.BlockSpec((block, width), lambda i, _: (i, 0)),
            scratch_shapes=[pltpu.VMEM((block, width), f32)],
        ),
        out_shape=jax.ShapeDtypeStruct((tokens, width), bf16),
    )(lane.reshape(1), *pieces, cotangent, resid_in, gain)


along_last = (((1,), (1,)), ((), ()))


def slot_pattern(block, at, count, capacity):
    slot = lax.broadcasted_iota(jnp.int32, (block, count), 0) + at
    low = lax.broadcasted_iota(jnp.int32, (block, count), 1) * capacity
    return ((slot >= low) & (slot < low + capacity)).astype(f32).astype(bf16)


def rows_kernel(lane_ref, routes_ref, share_ref, resid_ref, gain_ref, *refs):
    sent_ref, chooser_ref, rank_ref, high_ref, low_ref, normed_ref, turn_ref = refs
    tokens, quarter = normed_ref.shape
    experts = rank_ref.shape[1]
    block = chooser_ref.shape[0]
    capacity = 4 * tokens // experts
    step = pl.program_id(0)

    @pl.when(step == 0)
    def _():
        at = pl.ds(pl.multiple_of(lane_ref[0] * quarter, 128), quarter)
        some = 64

        def normalise(i, carry):
            rows = pl.ds(pl.multiple_of(i * some, some), some)
            wide = resid_ref[rows, :].astype(f32)
            inv_rms = lax.rsqrt(jnp.mean(wide * wide, axis=1, keepdims=True) + norm_eps)
            part = resid_ref[rows, at].astype(f32)
            normed_ref[rows, :] = (part * inv_rms * gain_ref[:, at]).astype(bf16)
            return carry

        lax.fori_loop(0, tokens // some, normalise, 0)
        ids = lax.broadcasted_iota(jnp.int32, (experts, tokens), 0)
        first = ids == routes_ref[0:1, :]
        second = ids == routes_ref[1:2, :]
        named = (first | second).astype(f32)
        share = jnp.where(first, share_ref[0:1, :], 0.0) + jnp.where(second, share_ref[1:2, :], 0.0)
        down = lax.broadcasted_iota(jnp.int32, (tokens, tokens), 0)
        over = lax.broadcasted_iota(jnp.int32, (tokens, tokens), 1)
        before = (down < over).astype(f32).astype(bf16)
        same = (over == down).astype(f32).astype(bf16)
        rank = jnp.dot(named.astype(bf16), before, preferred_element_type=f32)
        rank = jnp.where(named > 0.0, rank, -1.0).astype(bf16)
        turn_ref[...] = rank
        rank_ref[...] = lax.dot_general(
            same, rank, along_last, preferred_element_type=f32
        ).astype(bf16)
        high = share.astype(bf16)
        high_ref[...] = high
        low_ref[...] = (share - high.astype(f32)).astype(bf16)

    pattern = slot_pattern(block, step * block, experts, capacity)
    ranks = jnp.dot(pattern, turn_ref[...], preferred_element_type=f32)
    slot = lax.broadcasted_iota(jnp.int32, (block, 1), 0) + step * block
    wanted = lax.rem(slot, capacity).astype(f32)
    chooser = (ranks == wanted).astype(f32).astype(bf16)
    chooser_ref[...] = chooser
    sent_ref[...] = jnp.dot(chooser, normed_ref[...], preferred_element_type=f32).astype(bf16)


slot_block = 512


def chosen_rows(lane, routes, route_weights, resid_in, norm_gain, experts):
    tokens, width = resid_in.shape
    quarter = width // 4
    slots = 4 * tokens

    def whole(*shape):
        return pl.BlockSpec(shape, lambda i, _: (0, 0))

    return pl.pallas_call(
        rows_kernel,
        grid_spec=pltpu.PrefetchScalarGridSpec(
            num_scalar_prefetch=1,
            grid=(slots // slot_block,),
            in_specs=[whole(2, tokens), whole(2, tokens), whole(tokens, width), whole(1, width)],
            out_specs=[
                pl.BlockSpec((slot_block, quarter), lambda i, _: (i, 0)),
                pl.BlockSpec((slot_block, tokens), lambda i, _: (i, 0)),
                whole(tokens, experts),
                whole(experts, tokens),
                whole(experts, tokens),
            ],
            scratch_shapes=[pltpu.VMEM((tokens, quarter), bf16), pltpu.VMEM((experts, tokens), bf16)],
        ),
        out_shape=[
            jax.ShapeDtypeStruct((slots, quarter), bf16),
            jax.ShapeDtypeStruct((slots, tokens), bf16),
            jax.ShapeDtypeStruct((tokens, experts), bf16),
            jax.ShapeDtypeStruct((experts, tokens), bf16),
            jax.ShapeDtypeStruct((experts, tokens), bf16),
        ],
    )(lane.reshape(1), routes.T, route_weights.T, resid_in, norm_gain.reshape(1, width))


def weighted_kernel(chooser_ref, cot_ref, rank_ref, high_ref, low_ref, out_ref, token_ref):
    tokens, experts = rank_ref.shape
    block = chooser_ref.shape[0]
    capacity = 4 * tokens // experts
    at = pl.program_id(0) * block
    pattern = slot_pattern(block, at, experts, capacity)
    share = jnp.dot(pattern, high_ref[...], preferred_element_type=f32) + jnp.dot(
        pattern, low_ref[...], preferred_element_type=f32
    )
    chooser = chooser_ref[...]
    share = jnp.sum(share * chooser.astype(f32), axis=1, keepdims=True)
    width = out_ref.shape[1]
    part = 512
    for i in range(width // part):
        rows = jnp.dot(
            chooser, cot_ref[:, i * part : (i + 1) * part], preferred_element_type=f32
        )
        out_ref[:, i * part : (i + 1) * part] = (rows * share).astype(bf16)
    ranks = lax.dot_general(rank_ref[...], pattern, along_last, preferred_element_type=f32)
    slot = lax.broadcasted_iota(jnp.int32, (1, block), 1) + at
    token_ref[...] = (ranks == lax.rem(slot, capacity).astype(f32)).astype(f32).astype(bf16)


def weighted_rows(chooser, cotangent, rank, high, low):
    slots, tokens = chooser.shape
    width = cotangent.shape[1]

    def whole(array):
        return pl.BlockSpec(array.shape, lambda i: (0, 0))

    return pl.pallas_call(
        weighted_kernel,
        grid=(slots // slot_block,),
        in_specs=[pl.BlockSpec((slot_block, tokens), lambda i: (i, 0))]
        + [whole(x) for x in (cotangent, rank, high, low)],
        out_specs=[
            pl.BlockSpec((slot_block, width), lambda i: (i, 0)),
            pl.BlockSpec((tokens, slot_block), lambda i: (0, i)),
        ],
        out_shape=[
            jax.ShapeDtypeStruct((slots, width), bf16),
            jax.ShapeDtypeStruct((tokens, slots), bf16),
        ],
    )(chooser, cotangent, rank, high, low)


def write_parts(both, mat_ref, refs):
    part = lax.dot_general(both, mat_ref[...], along_last, preferred_element_type=f32)
    part = part.astype(bf16)
    at = 0
    for ref in refs:
        ref[...] = part[:, at : at + ref.shape[1]]
        at += ref.shape[1]


def first_kernel(cot_ref, act_ref, slope_ref, down_ref, mat_ref, both_ref, *refs):
    dhidden = lax.dot_general(
        cot_ref[...], down_ref[...], along_last, preferred_element_type=f32
    )
    dgate = (dhidden * slope_ref[...].astype(f32)).astype(bf16)
    dup = (dhidden * act_ref[...].astype(f32)).astype(bf16)
    both = jnp.concatenate([dgate, dup], axis=1)
    both_ref[...] = both
    write_parts(both, mat_ref, refs)


def other_kernel(both_ref, a_far_ref, b_far_ref, mat_ref, *refs):
    part = lax.dot_general(both_ref[...], mat_ref[...], along_last, preferred_element_type=f32)
    for i, ref in enumerate(refs):
        piece = part[:, i * direct_width : (i + 1) * direct_width]
        if i < 2:
            piece = piece + (a_far_ref, b_far_ref)[i][...].astype(f32)
        ref[...] = piece.astype(bf16)


part_block = 512


def by_rows(kernel, rowwise, matrices, sizes):
    slots = rowwise[0].shape[0]

    def rows(size):
        return pl.BlockSpec((part_block, size), lambda i: (i, 0))

    return pl.pallas_call(
        kernel,
        grid=(slots // part_block,),
        in_specs=[rows(x.shape[1]) for x in rowwise]
        + [pl.BlockSpec(x.shape, lambda i: (0, 0)) for x in matrices],
        out_specs=[rows(size) for size in sizes],
        out_shape=[jax.ShapeDtypeStruct((slots, size), bf16) for size in sizes],
    )(*rowwise, *matrices)


def on_device(
    resid_in,
    cotangent,
    norm_gain,
    routes,
    route_weights,
    gate_weight,
    up_weight,
    down_weight,
    out_weight,
    gate_b,
    gate_c,
    values_u,
    taps,
):
    token_count, model_width = resid_in.shape
    groups = lax.axis_size("sp")
    lanes = lax.axis_size("tp")
    lane = lax.axis_index("tp")
    expert_total = gate_weight.shape[0] * groups
    capacity = 4 * token_count // expert_total
    slots = expert_total * capacity
    quarter = model_width // lanes
    gate_mat, up_mat, down_mat = gate_weight[0], up_weight[0], down_weight[0]

    sent_rows, chooser, rank, high, low = chosen_rows(
        lane, routes, route_weights, resid_in, norm_gain, expert_total
    )
    got_part = exchanged(sent_rows.reshape(groups, capacity, quarter)).reshape(slots, quarter)
    sent_cots, token_chooser = weighted_rows(chooser, cotangent, rank, high, low)
    entry_cots = exchanged(sent_cots.reshape(groups, capacity, model_width))
    entry_cots = entry_cots.reshape(slots, model_width)
    entry_rows = placed_columns(lane, (got_part, ring_gather(got_part)), model_width)

    mixed = gate_c.astype(f32) * values_u.astype(f32)
    earlier = passed_along(mixed[-2:], "sp", 1)

    gate_pre = jnp.dot(entry_rows, gate_mat, preferred_element_type=f32)
    up_pre = jnp.dot(entry_rows, up_mat, preferred_element_type=f32)
    logistic = jax.nn.sigmoid(gate_pre)
    activated = gate_pre * logistic
    hidden = (activated * up_pre).astype(bf16)
    slope = up_pre * logistic * (1.0 + gate_pre * (1.0 - logistic))
    both_mat = jnp.concatenate([gate_mat, up_mat], axis=1)

    def weight_rows(further, first, count):
        at = ((lane + further) % lanes) * quarter + first * direct_width
        return lax.dynamic_slice_in_dim(both_mat, at, count * direct_width, axis=0)

    direct_mat = both_mat.reshape(lanes, quarter, -1)[:, -direct_width:]
    first_mat = jnp.concatenate(
        [weight_rows(2, 0, 2), weight_rows(3, 0, 1), weight_rows(1, 1, 1)]
        + [direct_mat.reshape(lanes * direct_width, -1)],
        axis=0,
    )
    other_mat = jnp.concatenate(
        [weight_rows(1, 0, 1), weight_rows(3, 1, 2), weight_rows(2, 2, 1)]
        + [weight_rows(0, 0, 3), weight_rows(1, 2, 1)],
        axis=0,
    )
    activated, slope, hidden, first_mat, other_mat = lax.optimization_barrier(
        (activated.astype(bf16), slope.astype(bf16), hidden, first_mat, other_mat)
    )
    dboth, a_far, b_far, a_behind, b_ahead, direct = by_rows(
        first_kernel,
        (entry_cots, activated, slope),
        (down_mat, first_mat),
        [both_mat.shape[1]] + [direct_width] * 4 + [lanes * direct_width],
    )

    def back(array):
        return exchanged(array.reshape(groups, capacity, -1)).reshape(slots, -1)

    def per_token(array):
        return jnp.dot(token_chooser, array, preferred_element_type=f32).astype(bf16)

    def plus(*arrays):
        return sum(array.astype(f32) for array in arrays).astype(bf16)

    a_far = turned(a_far, 1)
    b_far = turned(b_far, -1)
    direct = back(direct)
    a_next = turned(a_behind, -1)
    b_prev = turned(b_ahead, 1)
    a_ahead, b_behind, c_behind, c_far, a_own, b_own, c_own, c_ahead = by_rows(
        other_kernel, (dboth, a_far, b_far), (other_mat,), [direct_width] * 8
    )
    a_prev = turned(a_ahead, 1)
    b_next = turned(b_behind, -1)
    c_far = turned(c_far, 1)
    c_next = turned(c_behind, -1)
    c_ahead, direct = lax.optimization_barrier((c_ahead, direct))
    grad_down = jnp.einsum("rf,rd->fd", hidden, entry_cots, preferred_element_type=f32)
    wide = jnp.concatenate([plus(a_own, a_prev, a_next), plus(b_own, b_prev, b_next)], axis=1)
    c_own, wide = lax.optimization_barrier((c_own, wide))
    wide = back(wide)
    direct_parts = lane_gather(per_token(direct))
    c_prev = turned(plus(c_ahead, c_far), 1)
    narrow = back(plus(c_own, c_prev, c_next))
    wide_parts = lane_gather(per_token(wide))
    narrow_parts = lane_gather(per_token(narrow))
    pieces = (*wide_parts, *narrow_parts, *direct_parts)
    grad_resid = finish(lane, pieces, cotangent, resid_in, norm_gain)

    extended = jnp.concatenate([earlier, mixed], axis=0)
    conv = (
        taps[0] * extended[:token_count]
        + taps[1] * extended[1 : token_count + 1]
        + taps[2] * extended[2 : token_count + 2]
    )
    merged = (gate_b.astype(f32) * conv).astype(bf16)
    out_parts = jnp.einsum("td,tc->dc", grad_resid, merged, preferred_element_type=f32).astype(bf16)
    out_tiles = exchanged(out_parts.reshape(groups, model_width // groups, -1))
    grad_out_weight = jnp.sum(out_tiles.astype(f32), axis=0)
    late_both, out_parts = lax.optimization_barrier((dboth, out_parts))
    grad_both = jnp.einsum("rd,rf->df", entry_rows, late_both, preferred_element_type=f32)
    late_resid, grad_both = lax.optimization_barrier((grad_resid, grad_both))
    grad_gate, grad_up = jnp.split(grad_both, 2, axis=1)
    dmerged = jnp.dot(late_resid, out_weight, preferred_element_type=f32)
    grad_gate_b = (dmerged * conv).astype(bf16)
    dconv = dmerged * gate_b.astype(f32)
    later = passed_along(dconv[:2], "sp", -1)
    extended_grad = jnp.concatenate([dconv, later], axis=0)
    dmixed = (
        taps[2] * extended_grad[:token_count]
        + taps[1] * extended_grad[1 : token_count + 1]
        + taps[0] * extended_grad[2 : token_count + 2]
    )
    grad_gate_c = (dmixed * values_u.astype(f32)).astype(bf16)
    grad_values = (dmixed * gate_c.astype(f32)).astype(bf16)
    return (
        grad_gate[None],
        grad_up[None],
        grad_down[None],
        grad_resid,
        grad_out_weight,
        grad_gate_b,
        grad_gate_c,
        grad_values,
    )


def solution(mesh):
    placed = (
        P("sp", None),
        P("sp", None),
        P(),
        P("sp", None),
        P("sp", None),
        P("sp", None, "tp"),
        P("sp", None, "tp"),
        P("sp", "tp", None),
        P(None, "tp"),
        P("sp", "tp"),
        P("sp", "tp"),
        P("sp", "tp"),
        P(None, "tp"),
    )

    return jax.shard_map(
        on_device,
        mesh=mesh,
        in_specs=placed,
        out_specs=(
            P("sp", None, "tp"),
            P("sp", None, "tp"),
            P("sp", "tp", None),
            P("sp", None),
            P("sp", "tp"),
            P("sp", "tp"),
            P("sp", "tp"),
            P("sp", "tp"),
        ),
        check_vma=False,
    )
```

```python
import jax
import jax.numpy as jnp
from jax import lax
from jax.experimental import pallas as pl
from jax.experimental.pallas import tpu as pltpu
from jax.sharding import PartitionSpec as P

norm_eps = 1e-06
direct_width = 128
f32 = jnp.float32
bf16 = jnp.bfloat16


def passed_along(array, axis, by):
    size = lax.axis_size(axis)
    pairs = [(i, i + by) for i in range(size) if 0 <= i + by < size]
    return lax.ppermute(array, axis, pairs)


def turned(array, by):
    size = lax.axis_size("tp")
    return lax.ppermute(array, "tp", [(i, (i + by) % size) for i in range(size)])


def exchanged(array):
    return lax.all_to_all(array, "sp", split_axis=0, concat_axis=0, tiled=True)


def ring_gather(piece):
    half = piece.shape[0] // 2
    prev = turned(piece, 1)
    nxt = turned(piece, -1)
    far_top = turned(prev[:half], 1)
    far_low = turned(nxt[half:], -1)
    return prev, nxt, far_top, far_low


def placed_columns(lane, pieces, width):
    piece, (prev, nxt, far_top, far_low) = pieces
    half = piece.shape[0] // 2
    size = piece.shape[1]
    lanes = width // size
    whole = jnp.zeros((piece.shape[0], width), piece.dtype)
    whole = lax.dynamic_update_slice(whole, piece, (0, lane * size))
    whole = lax.dynamic_update_slice(whole, prev, (0, ((lane + lanes - 1) % lanes) * size))
    whole = lax.dynamic_update_slice(whole, nxt, (0, ((lane + 1) % lanes) * size))
    far = ((lane + 2) % lanes) * size
    whole = lax.dynamic_update_slice(whole, far_top, (0, far))
    return lax.dynamic_update_slice(whole, far_low, (half, far))


def lane_gather(piece):
    others = []
    for way in (1, -1, 2):
        others.append(turned(piece, way))
    return piece, *others


lane_steps = (0, -1, 1, 2)


def finish_kernel(lane_ref, *refs):
    wide_refs, narrow_refs, direct_refs = refs[:4], refs[4:8], refs[8:12]
    cot_ref, resid_ref, gain_ref, out_ref, grad_ref = refs[12:]
    width = grad_ref.shape[1]
    quarter = width // 4
    wide = wide_refs[0].shape[1]
    for step, wide_ref, narrow_ref in zip(lane_steps, wide_refs, narrow_refs):
        start = ((lane_ref[0] + (4 + step)) % 4) * quarter
        grad_ref[:, pl.ds(pl.multiple_of(start, 128), wide)] = wide_ref[...].astype(f32)
        grad_ref[:, pl.ds(pl.multiple_of(start + wide, 128), direct_width)] = narrow_ref[
            ...
        ].astype(f32)
    direct = sum(ref[...].astype(f32) for ref in direct_refs)
    for place in range(4):
        end = (place + 1) * quarter
        grad_ref[:, end - direct_width : end] = direct[
            :, place * direct_width : (place + 1) * direct_width
        ]
    resid = resid_ref[...].astype(f32)
    inv_rms = lax.rsqrt(jnp.mean(resid * resid, axis=1, keepdims=True) + norm_eps)
    scaled = grad_ref[...] * gain_ref[...]
    inner = jnp.mean(scaled * resid, axis=1, keepdims=True)
    out_ref[...] = (
        cot_ref[...].astype(f32) + inv_rms * scaled - resid * (inv_rms**3 * inner)
    ).astype(bf16)


def finish(lane, pieces, cotangent, resid_in, norm_gain):
    tokens, width = cotangent.shape
    block = 192

    def rows(array):
        return pl.BlockSpec((block, array.shape[1]), lambda i, _: (i, 0))

    gain = norm_gain.reshape(1, width)
    return pl.pallas_call(
        finish_kernel,
        grid_spec=pltpu.PrefetchScalarGridSpec(
            num_scalar_prefetch=1,
            grid=(tokens // block,),
            in_specs=[rows(x) for x in (*pieces, cotangent, resid_in)]
            + [pl.BlockSpec((1, width), lambda i, _: (0, 0))],
            out_specs=pl.BlockSpec((block, width), lambda i, _: (i, 0)),
            scratch_shapes=[pltpu.VMEM((block, width), f32)],
        ),
        out_shape=jax.ShapeDtypeStruct((tokens, width), bf16),
    )(lane.reshape(1), *pieces, cotangent, resid_in, gain)


along_last = (((1,), (1,)), ((), ()))


def slot_pattern(block, at, count, capacity):
    slot = lax.broadcasted_iota(jnp.int32, (block, count), 0) + at
    low = lax.broadcasted_iota(jnp.int32, (block, count), 1) * capacity
    return ((slot >= low) & (slot < low + capacity)).astype(f32).astype(bf16)


def rows_kernel(lane_ref, routes_ref, share_ref, resid_ref, gain_ref, *refs):
    sent_ref, chooser_ref, rank_ref, high_ref, low_ref, normed_ref, turn_ref = refs
    tokens, quarter = normed_ref.shape
    experts = rank_ref.shape[1]
    block = chooser_ref.shape[0]
    capacity = 4 * tokens // experts
    step = pl.program_id(0)

    @pl.when(step == 0)
    def _():
        at = pl.ds(pl.multiple_of(lane_ref[0] * quarter, 128), quarter)
        some = 64

        def normalise(i, carry):
            rows = pl.ds(pl.multiple_of(i * some, some), some)
            wide = resid_ref[rows, :].astype(f32)
            inv_rms = lax.rsqrt(jnp.mean(wide * wide, axis=1, keepdims=True) + norm_eps)
            part = resid_ref[rows, at].astype(f32)
            normed_ref[rows, :] = (part * inv_rms * gain_ref[:, at]).astype(bf16)
            return carry

        lax.fori_loop(0, tokens // some, normalise, 0)
        ids = lax.broadcasted_iota(jnp.int32, (experts, tokens), 0)
        first = ids == routes_ref[0:1, :]
        second = ids == routes_ref[1:2, :]
        named = (first | second).astype(f32)
        share = jnp.where(first, share_ref[0:1, :], 0.0) + jnp.where(second, share_ref[1:2, :], 0.0)
        down = lax.broadcasted_iota(jnp.int32, (tokens, tokens), 0)
        over = lax.broadcasted_iota(jnp.int32, (tokens, tokens), 1)
        before = (down < over).astype(f32).astype(bf16)
        same = (over == down).astype(f32).astype(bf16)
        rank = jnp.dot(named.astype(bf16), before, preferred_element_type=f32)
        rank = jnp.where(named > 0.0, rank, -1.0).astype(bf16)
        turn_ref[...] = rank
        rank_ref[...] = lax.dot_general(
            same, rank, along_last, preferred_element_type=f32
        ).astype(bf16)
        high = share.astype(bf16)
        high_ref[...] = high
        low_ref[...] = (share - high.astype(f32)).astype(bf16)

    pattern = slot_pattern(block, step * block, experts, capacity)
    ranks = jnp.dot(pattern, turn_ref[...], preferred_element_type=f32)
    slot = lax.broadcasted_iota(jnp.int32, (block, 1), 0) + step * block
    wanted = lax.rem(slot, capacity).astype(f32)
    chooser = (ranks == wanted).astype(f32).astype(bf16)
    chooser_ref[...] = chooser
    sent_ref[...] = jnp.dot(chooser, normed_ref[...], preferred_element_type=f32).astype(bf16)


slot_block = 512


def chosen_rows(lane, routes, route_weights, resid_in, norm_gain, experts):
    tokens, width = resid_in.shape
    quarter = width // 4
    slots = 4 * tokens

    def whole(*shape):
        return pl.BlockSpec(shape, lambda i, _: (0, 0))

    return pl.pallas_call(
        rows_kernel,
        grid_spec=pltpu.PrefetchScalarGridSpec(
            num_scalar_prefetch=1,
            grid=(slots // slot_block,),
            in_specs=[whole(2, tokens), whole(2, tokens), whole(tokens, width), whole(1, width)],
            out_specs=[
                pl.BlockSpec((slot_block, quarter), lambda i, _: (i, 0)),
                pl.BlockSpec((slot_block, tokens), lambda i, _: (i, 0)),
                whole(tokens, experts),
                whole(experts, tokens),
                whole(experts, tokens),
            ],
            scratch_shapes=[pltpu.VMEM((tokens, quarter), bf16), pltpu.VMEM((experts, tokens), bf16)],
        ),
        out_shape=[
            jax.ShapeDtypeStruct((slots, quarter), bf16),
            jax.ShapeDtypeStruct((slots, tokens), bf16),
            jax.ShapeDtypeStruct((tokens, experts), bf16),
            jax.ShapeDtypeStruct((experts, tokens), bf16),
            jax.ShapeDtypeStruct((experts, tokens), bf16),
        ],
    )(lane.reshape(1), routes.T, route_weights.T, resid_in, norm_gain.reshape(1, width))


def weighted_kernel(chooser_ref, cot_ref, rank_ref, high_ref, low_ref, out_ref, token_ref):
    tokens, experts = rank_ref.shape
    block = chooser_ref.shape[0]
    capacity = 4 * tokens // experts
    at = pl.program_id(0) * block
    pattern = slot_pattern(block, at, experts, capacity)
    share = jnp.dot(pattern, high_ref[...], preferred_element_type=f32) + jnp.dot(
        pattern, low_ref[...], preferred_element_type=f32
    )
    chooser = chooser_ref[...]
    share = jnp.sum(share * chooser.astype(f32), axis=1, keepdims=True)
    width = out_ref.shape[1]
    part = 512
    for i in range(width // part):
        rows = jnp.dot(
            chooser, cot_ref[:, i * part : (i + 1) * part], preferred_element_type=f32
        )
        out_ref[:, i * part : (i + 1) * part] = (rows * share).astype(bf16)
    ranks = lax.dot_general(rank_ref[...], pattern, along_last, preferred_element_type=f32)
    slot = lax.broadcasted_iota(jnp.int32, (1, block), 1) + at
    token_ref[...] = (ranks == lax.rem(slot, capacity).astype(f32)).astype(f32).astype(bf16)


def weighted_rows(chooser, cotangent, rank, high, low):
    slots, tokens = chooser.shape
    width = cotangent.shape[1]

    def whole(array):
        return pl.BlockSpec(array.shape, lambda i: (0, 0))

    return pl.pallas_call(
        weighted_kernel,
        grid=(slots // slot_block,),
        in_specs=[pl.BlockSpec((slot_block, tokens), lambda i: (i, 0))]
        + [whole(x) for x in (cotangent, rank, high, low)],
        out_specs=[
            pl.BlockSpec((slot_block, width), lambda i: (i, 0)),
            pl.BlockSpec((tokens, slot_block), lambda i: (0, i)),
        ],
        out_shape=[
            jax.ShapeDtypeStruct((slots, width), bf16),
            jax.ShapeDtypeStruct((tokens, slots), bf16),
        ],
    )(chooser, cotangent, rank, high, low)


def write_parts(both, mat_ref, refs):
    part = lax.dot_general(both, mat_ref[...], along_last, preferred_element_type=f32)
    part = part.astype(bf16)
    at = 0
    for ref in refs:
        ref[...] = part[:, at : at + ref.shape[1]]
        at += ref.shape[1]


def first_kernel(cot_ref, act_ref, slope_ref, down_ref, mat_ref, both_ref, *refs):
    dhidden = lax.dot_general(
        cot_ref[...], down_ref[...], along_last, preferred_element_type=f32
    )
    dgate = (dhidden * slope_ref[...].astype(f32)).astype(bf16)
    dup = (dhidden * act_ref[...].astype(f32)).astype(bf16)
    both = jnp.concatenate([dgate, dup], axis=1)
    both_ref[...] = both
    write_parts(both, mat_ref, refs)


def other_kernel(both_ref, a_far_ref, b_far_ref, mat_ref, *refs):
    part = lax.dot_general(both_ref[...], mat_ref[...], along_last, preferred_element_type=f32)
    at = 0
    for i, ref in enumerate(refs):
        piece = part[:, at : at + ref.shape[1]]
        at += ref.shape[1]
        if i < 2:
            piece = piece + (a_far_ref, b_far_ref)[i][...].astype(f32)
        ref[...] = piece.astype(bf16)


def wide_kernel(own_ref, a_prev_ref, a_next_ref, b_prev_ref, b_next_ref, out_ref):
    for at, refs in ((0, (a_prev_ref, a_next_ref)), (direct_width, (b_prev_ref, b_next_ref))):
        columns = slice(at, at + direct_width)
        total = own_ref[:, columns].astype(f32) + refs[0][...].astype(f32)
        out_ref[:, columns] = (total + refs[1][...].astype(f32)).astype(bf16)


part_block = 512


def by_rows(kernel, rowwise, matrices, sizes):
    slots = rowwise[0].shape[0]

    def rows(size):
        return pl.BlockSpec((part_block, size), lambda i: (i, 0))

    return pl.pallas_call(
        kernel,
        grid=(slots // part_block,),
        in_specs=[rows(x.shape[1]) for x in rowwise]
        + [pl.BlockSpec(x.shape, lambda i: (0, 0)) for x in matrices],
        out_specs=[rows(size) for size in sizes],
        out_shape=[jax.ShapeDtypeStruct((slots, size), bf16) for size in sizes],
    )(*rowwise, *matrices)


def on_device(
    resid_in,
    cotangent,
    norm_gain,
    routes,
    route_weights,
    gate_weight,
    up_weight,
    down_weight,
    out_weight,
    gate_b,
    gate_c,
    values_u,
    taps,
):
    token_count, model_width = resid_in.shape
    groups = lax.axis_size("sp")
    lanes = lax.axis_size("tp")
    lane = lax.axis_index("tp")
    expert_total = gate_weight.shape[0] * groups
    capacity = 4 * token_count // expert_total
    slots = expert_total * capacity
    quarter = model_width // lanes
    gate_mat, up_mat, down_mat = gate_weight[0], up_weight[0], down_weight[0]

    sent_rows, chooser, rank, high, low = chosen_rows(
        lane, routes, route_weights, resid_in, norm_gain, expert_total
    )
    got_part = exchanged(sent_rows.reshape(groups, capacity, quarter)).reshape(slots, quarter)
    sent_cots, token_chooser = weighted_rows(chooser, cotangent, rank, high, low)
    entry_cots = exchanged(sent_cots.reshape(groups, capacity, model_width))
    entry_cots = entry_cots.reshape(slots, model_width)
    entry_rows = placed_columns(lane, (got_part, ring_gather(got_part)), model_width)

    mixed = gate_c.astype(f32) * values_u.astype(f32)
    earlier = passed_along(mixed[-2:], "sp", 1)

    gate_pre = jnp.dot(entry_rows, gate_mat, preferred_element_type=f32)
    up_pre = jnp.dot(entry_rows, up_mat, preferred_element_type=f32)
    logistic = jax.nn.sigmoid(gate_pre)
    activated = gate_pre * logistic
    hidden = (activated * up_pre).astype(bf16)
    slope = up_pre * logistic * (1.0 + gate_pre * (1.0 - logistic))
    both_mat = jnp.concatenate([gate_mat, up_mat], axis=1)

    def weight_rows(further, first, count):
        at = ((lane + further) % lanes) * quarter + first * direct_width
        return lax.dynamic_slice_in_dim(both_mat, at, count * direct_width, axis=0)

    direct_mat = both_mat.reshape(lanes, quarter, -1)[:, -direct_width:]
    first_mat = jnp.concatenate(
        [weight_rows(2, 0, 2), weight_rows(3, 0, 1), weight_rows(1, 1, 1)]
        + [direct_mat.reshape(lanes * direct_width, -1)],
        axis=0,
    )
    other_mat = jnp.concatenate(
        [weight_rows(1, 0, 1), weight_rows(3, 1, 2), weight_rows(2, 2, 1)]
        + [weight_rows(0, 0, 3), weight_rows(1, 2, 1)],
        axis=0,
    )
    activated, slope, hidden, first_mat, other_mat = lax.optimization_barrier(
        (activated.astype(bf16), slope.astype(bf16), hidden, first_mat, other_mat)
    )
    dboth, a_far, b_far, a_behind, b_ahead, direct = by_rows(
        first_kernel,
        (entry_cots, activated, slope),
        (down_mat, first_mat),
        [both_mat.shape[1]] + [direct_width] * 4 + [lanes * direct_width],
    )

    def back(array):
        return exchanged(array.reshape(groups, capacity, -1)).reshape(slots, -1)

    def per_token(array):
        return jnp.dot(token_chooser, array, preferred_element_type=f32).astype(bf16)

    def plus(*arrays):
        return sum(array.astype(f32) for array in arrays).astype(bf16)

    a_far = turned(a_far, 1)
    b_far = turned(b_far, -1)
    direct = back(direct)
    a_next = turned(a_behind, -1)
    b_prev = turned(b_ahead, 1)
    sizes = [direct_width] * 4 + [2 * direct_width] + [direct_width] * 2
    a_ahead, b_behind, c_behind, c_far, wide_own, c_own, c_ahead = by_rows(
        other_kernel, (dboth, a_far, b_far), (other_mat,), sizes
    )
    a_prev = turned(a_ahead, 1)
    b_next = turned(b_behind, -1)
    c_far = turned(c_far, 1)
    c_next = turned(c_behind, -1)
    c_ahead, direct = lax.optimization_barrier((c_ahead, direct))
    grad_down = jnp.einsum("rf,rd->fd", hidden, entry_cots, preferred_element_type=f32)
    (wide,) = by_rows(
        wide_kernel, (wide_own, a_prev, a_next, b_prev, b_next), (), [2 * direct_width]
    )
    c_own, wide = lax.optimization_barrier((c_own, wide))
    wide = back(wide)
    direct_parts = lane_gather(per_token(direct))
    c_prev = turned(plus(c_ahead, c_far), 1)
    narrow = back(plus(c_own, c_prev, c_next))
    wide_parts = lane_gather(per_token(wide))
    narrow_parts = lane_gather(per_token(narrow))
    pieces = (*wide_parts, *narrow_parts, *direct_parts)
    grad_resid = finish(lane, pieces, cotangent, resid_in, norm_gain)

    extended = jnp.concatenate([earlier, mixed], axis=0)
    conv = (
        taps[0] * extended[:token_count]
        + taps[1] * extended[1 : token_count + 1]
        + taps[2] * extended[2 : token_count + 2]
    )
    merged = (gate_b.astype(f32) * conv).astype(bf16)
    out_parts = jnp.einsum("td,tc->dc", grad_resid, merged, preferred_element_type=f32).astype(bf16)
    out_tiles = exchanged(out_parts.reshape(groups, model_width // groups, -1))
    grad_out_weight = jnp.sum(out_tiles.astype(f32), axis=0)
    late_both, out_parts = lax.optimization_barrier((dboth, out_parts))
    grad_both = jnp.einsum("rd,rf->df", entry_rows, late_both, preferred_element_type=f32)
    late_resid, grad_both = lax.optimization_barrier((grad_resid, grad_both))
    grad_gate, grad_up = jnp.split(grad_both, 2, axis=1)
    dmerged = jnp.dot(late_resid, out_weight, preferred_element_type=f32)
    grad_gate_b = (dmerged * conv).astype(bf16)
    dconv = dmerged * gate_b.astype(f32)
    later = passed_along(dconv[:2], "sp", -1)
    extended_grad = jnp.concatenate([dconv, later], axis=0)
    dmixed = (
        taps[2] * extended_grad[:token_count]
        + taps[1] * extended_grad[1 : token_count + 1]
        + taps[0] * extended_grad[2 : token_count + 2]
    )
    grad_gate_c = (dmixed * values_u.astype(f32)).astype(bf16)
    grad_values = (dmixed * gate_c.astype(f32)).astype(bf16)
    return (
        grad_gate[None],
        grad_up[None],
        grad_down[None],
        grad_resid,
        grad_out_weight,
        grad_gate_b,
        grad_gate_c,
        grad_values,
    )


def solution(mesh):
    placed = (
        P("sp", None),
        P("sp", None),
        P(),
        P("sp", None),
        P("sp", None),
        P("sp", None, "tp"),
        P("sp", None, "tp"),
        P("sp", "tp", None),
        P(None, "tp"),
        P("sp", "tp"),
        P("sp", "tp"),
        P("sp", "tp"),
        P(None, "tp"),
    )

    return jax.shard_map(
        on_device,
        mesh=mesh,
        in_specs=placed,
        out_specs=(
            P("sp", None, "tp"),
            P("sp", None, "tp"),
            P("sp", "tp", None),
            P("sp", None),
            P("sp", "tp"),
            P("sp", "tp"),
            P("sp", "tp"),
            P("sp", "tp"),
        ),
        check_vma=False,
    )
```

```python
import jax
import jax.numpy as jnp
from jax import lax
from jax.experimental import pallas as pl
from jax.experimental.pallas import tpu as pltpu
from jax.sharding import PartitionSpec as P

norm_eps = 1e-06
direct_width = 128
f32 = jnp.float32
bf16 = jnp.bfloat16


def passed_along(array, axis, by):
    size = lax.axis_size(axis)
    pairs = [(i, i + by) for i in range(size) if 0 <= i + by < size]
    return lax.ppermute(array, axis, pairs)


def turned(array, by):
    size = lax.axis_size("tp")
    return lax.ppermute(array, "tp", [(i, (i + by) % size) for i in range(size)])


def exchanged(array):
    return lax.all_to_all(array, "sp", split_axis=0, concat_axis=0, tiled=True)


def ring_gather(piece):
    half = piece.shape[0] // 2
    prev = turned(piece, 1)
    nxt = turned(piece, -1)
    far_top = turned(prev[:half], 1)
    far_low = turned(nxt[half:], -1)
    return prev, nxt, far_top, far_low


def placed_columns(lane, pieces, width):
    piece, (prev, nxt, far_top, far_low) = pieces
    half = piece.shape[0] // 2
    size = piece.shape[1]
    lanes = width // size
    whole = jnp.zeros((piece.shape[0], width), piece.dtype)
    whole = lax.dynamic_update_slice(whole, piece, (0, lane * size))
    whole = lax.dynamic_update_slice(whole, prev, (0, ((lane + lanes - 1) % lanes) * size))
    whole = lax.dynamic_update_slice(whole, nxt, (0, ((lane + 1) % lanes) * size))
    far = ((lane + 2) % lanes) * size
    whole = lax.dynamic_update_slice(whole, far_top, (0, far))
    return lax.dynamic_update_slice(whole, far_low, (half, far))


def lane_gather(piece):
    others = []
    for way in (1, -1, 2):
        others.append(turned(piece, way))
    return piece, *others


lane_steps = (0, -1, 1, 2)


def finish_kernel(lane_ref, *refs):
    wide_refs, narrow_refs, direct_refs = refs[:4], refs[4:8], refs[8:12]
    cot_ref, resid_ref, gain_ref, out_ref, grad_ref = refs[12:]
    width = grad_ref.shape[1]
    quarter = width // 4
    wide = wide_refs[0].shape[1]
    for step, wide_ref, narrow_ref in zip(lane_steps, wide_refs, narrow_refs):
        start = ((lane_ref[0] + (4 + step)) % 4) * quarter
        grad_ref[:, pl.ds(pl.multiple_of(start, 128), wide)] = wide_ref[...].astype(f32)
        grad_ref[:, pl.ds(pl.multiple_of(start + wide, 128), direct_width)] = narrow_ref[
            ...
        ].astype(f32)
    direct = sum(ref[...].astype(f32) for ref in direct_refs)
    for place in range(4):
        end = (place + 1) * quarter
        grad_ref[:, end - direct_width : end] = direct[
            :, place * direct_width : (place + 1) * direct_width
        ]
    resid = resid_ref[...].astype(f32)
    inv_rms = lax.rsqrt(jnp.mean(resid * resid, axis=1, keepdims=True) + norm_eps)
    scaled = grad_ref[...] * gain_ref[...]
    inner = jnp.mean(scaled * resid, axis=1, keepdims=True)
    out_ref[...] = (
        cot_ref[...].astype(f32) + inv_rms * scaled - resid * (inv_rms**3 * inner)
    ).astype(bf16)


def finish(lane, pieces, cotangent, resid_in, norm_gain):
    tokens, width = cotangent.shape
    block = 192

    def rows(array):
        return pl.BlockSpec((block, array.shape[1]), lambda i, _: (i, 0))

    gain = norm_gain.reshape(1, width)
    return pl.pallas_call(
        finish_kernel,
        grid_spec=pltpu.PrefetchScalarGridSpec(
            num_scalar_prefetch=1,
            grid=(tokens // block,),
            in_specs=[rows(x) for x in (*pieces, cotangent, resid_in)]
            + [pl.BlockSpec((1, width), lambda i, _: (0, 0))],
            out_specs=pl.BlockSpec((block, width), lambda i, _: (i, 0)),
            scratch_shapes=[pltpu.VMEM((block, width), f32)],
        ),
        out_shape=jax.ShapeDtypeStruct((tokens, width), bf16),
    )(lane.reshape(1), *pieces, cotangent, resid_in, gain)


along_last = (((1,), (1,)), ((), ()))


def slot_pattern(block, at, count, capacity):
    slot = lax.broadcasted_iota(jnp.int32, (block, count), 0) + at
    low = lax.broadcasted_iota(jnp.int32, (block, count), 1) * capacity
    return ((slot >= low) & (slot < low + capacity)).astype(f32).astype(bf16)


def rows_kernel(lane_ref, routes_ref, share_ref, resid_ref, gain_ref, *refs):
    sent_ref, chooser_ref, rank_ref, high_ref, low_ref, normed_ref, turn_ref = refs
    tokens, quarter = normed_ref.shape
    experts = rank_ref.shape[1]
    block = chooser_ref.shape[0]
    capacity = 4 * tokens // experts
    step = pl.program_id(0)

    @pl.when(step == 0)
    def _():
        at = pl.ds(pl.multiple_of(lane_ref[0] * quarter, 128), quarter)
        some = 64

        def normalise(i, carry):
            rows = pl.ds(pl.multiple_of(i * some, some), some)
            wide = resid_ref[rows, :].astype(f32)
            inv_rms = lax.rsqrt(jnp.mean(wide * wide, axis=1, keepdims=True) + norm_eps)
            part = resid_ref[rows, at].astype(f32)
            normed_ref[rows, :] = (part * inv_rms * gain_ref[:, at]).astype(bf16)
            return carry

        lax.fori_loop(0, tokens // some, normalise, 0)
        ids = lax.broadcasted_iota(jnp.int32, (experts, tokens), 0)
        first = ids == routes_ref[0:1, :]
        second = ids == routes_ref[1:2, :]
        named = (first | second).astype(f32)
        share = jnp.where(first, share_ref[0:1, :], 0.0) + jnp.where(second, share_ref[1:2, :], 0.0)
        down = lax.broadcasted_iota(jnp.int32, (tokens, tokens), 0)
        over = lax.broadcasted_iota(jnp.int32, (tokens, tokens), 1)
        before = (down < over).astype(f32).astype(bf16)
        same = (over == down).astype(f32).astype(bf16)
        rank = jnp.dot(named.astype(bf16), before, preferred_element_type=f32)
        rank = jnp.where(named > 0.0, rank, -1.0).astype(bf16)
        turn_ref[...] = rank
        rank_ref[...] = lax.dot_general(
            same, rank, along_last, preferred_element_type=f32
        ).astype(bf16)
        high = share.astype(bf16)
        high_ref[...] = high
        low_ref[...] = (share - high.astype(f32)).astype(bf16)

    pattern = slot_pattern(block, step * block, experts, capacity)
    ranks = jnp.dot(pattern, turn_ref[...], preferred_element_type=f32)
    slot = lax.broadcasted_iota(jnp.int32, (block, 1), 0) + step * block
    wanted = lax.rem(slot, capacity).astype(f32)
    chooser = (ranks == wanted).astype(f32).astype(bf16)
    chooser_ref[...] = chooser
    sent_ref[...] = jnp.dot(chooser, normed_ref[...], preferred_element_type=f32).astype(bf16)


slot_block = 512


def chosen_rows(lane, routes, route_weights, resid_in, norm_gain, experts):
    tokens, width = resid_in.shape
    quarter = width // 4
    slots = 4 * tokens

    def whole(*shape):
        return pl.BlockSpec(shape, lambda i, _: (0, 0))

    return pl.pallas_call(
        rows_kernel,
        grid_spec=pltpu.PrefetchScalarGridSpec(
            num_scalar_prefetch=1,
            grid=(slots // slot_block,),
            in_specs=[whole(2, tokens), whole(2, tokens), whole(tokens, width), whole(1, width)],
            out_specs=[
                pl.BlockSpec((slot_block, quarter), lambda i, _: (i, 0)),
                pl.BlockSpec((slot_block, tokens), lambda i, _: (i, 0)),
                whole(tokens, experts),
                whole(experts, tokens),
                whole(experts, tokens),
            ],
            scratch_shapes=[pltpu.VMEM((tokens, quarter), bf16), pltpu.VMEM((experts, tokens), bf16)],
        ),
        out_shape=[
            jax.ShapeDtypeStruct((slots, quarter), bf16),
            jax.ShapeDtypeStruct((slots, tokens), bf16),
            jax.ShapeDtypeStruct((tokens, experts), bf16),
            jax.ShapeDtypeStruct((experts, tokens), bf16),
            jax.ShapeDtypeStruct((experts, tokens), bf16),
        ],
    )(lane.reshape(1), routes.T, route_weights.T, resid_in, norm_gain.reshape(1, width))


def weighted_kernel(chooser_ref, cot_ref, rank_ref, high_ref, low_ref, out_ref, token_ref):
    tokens, experts = rank_ref.shape
    block = chooser_ref.shape[0]
    capacity = 4 * tokens // experts
    at = pl.program_id(0) * block
    pattern = slot_pattern(block, at, experts, capacity)
    share = jnp.dot(pattern, high_ref[...], preferred_element_type=f32) + jnp.dot(
        pattern, low_ref[...], preferred_element_type=f32
    )
    chooser = chooser_ref[...]
    share = jnp.sum(share * chooser.astype(f32), axis=1, keepdims=True)
    width = out_ref.shape[1]
    part = 512
    for i in range(width // part):
        rows = jnp.dot(
            chooser, cot_ref[:, i * part : (i + 1) * part], preferred_element_type=f32
        )
        out_ref[:, i * part : (i + 1) * part] = (rows * share).astype(bf16)
    ranks = lax.dot_general(rank_ref[...], pattern, along_last, preferred_element_type=f32)
    slot = lax.broadcasted_iota(jnp.int32, (1, block), 1) + at
    token_ref[...] = (ranks == lax.rem(slot, capacity).astype(f32)).astype(f32).astype(bf16)


def weighted_rows(chooser, cotangent, rank, high, low):
    slots, tokens = chooser.shape
    width = cotangent.shape[1]

    def whole(array):
        return pl.BlockSpec(array.shape, lambda i: (0, 0))

    return pl.pallas_call(
        weighted_kernel,
        grid=(slots // slot_block,),
        in_specs=[pl.BlockSpec((slot_block, tokens), lambda i: (i, 0))]
        + [whole(x) for x in (cotangent, rank, high, low)],
        out_specs=[
            pl.BlockSpec((slot_block, width), lambda i: (i, 0)),
            pl.BlockSpec((tokens, slot_block), lambda i: (0, i)),
        ],
        out_shape=[
            jax.ShapeDtypeStruct((slots, width), bf16),
            jax.ShapeDtypeStruct((tokens, slots), bf16),
        ],
    )(chooser, cotangent, rank, high, low)


def write_parts(both, mat_ref, refs):
    part = lax.dot_general(both, mat_ref[...], along_last, preferred_element_type=f32)
    part = part.astype(bf16)
    at = 0
    for ref in refs:
        ref[...] = part[:, at : at + ref.shape[1]]
        at += ref.shape[1]


def first_kernel(cot_ref, act_ref, slope_ref, down_ref, mat_ref, both_ref, *refs):
    dhidden = lax.dot_general(
        cot_ref[...], down_ref[...], along_last, preferred_element_type=f32
    )
    dgate = (dhidden * slope_ref[...].astype(f32)).astype(bf16)
    dup = (dhidden * act_ref[...].astype(f32)).astype(bf16)
    both = jnp.concatenate([dgate, dup], axis=1)
    both_ref[...] = both
    write_parts(both, mat_ref, refs)


def other_kernel(both_ref, a_next_ref, b_prev_ref, mat_ref, own_ref, *refs):
    part = lax.dot_general(both_ref[...], mat_ref[...], along_last, preferred_element_type=f32)
    for i, ref in enumerate((a_next_ref, b_prev_ref)):
        at = slice(i * direct_width, (i + 1) * direct_width)
        own_ref[:, at] = (part[:, at] + ref[...].astype(f32)).astype(bf16)
    for i, ref in enumerate(refs):
        ref[...] = part[:, (i + 2) * direct_width : (i + 3) * direct_width].astype(bf16)


def wide_kernel(own_ref, a_prev_ref, b_next_ref, out_ref):
    for i, ref in enumerate((a_prev_ref, b_next_ref)):
        at = slice(i * direct_width, (i + 1) * direct_width)
        out_ref[:, at] = (own_ref[:, at].astype(f32) + ref[...].astype(f32)).astype(bf16)


part_block = 512


def by_rows(kernel, rowwise, matrices, sizes):
    slots = rowwise[0].shape[0]

    def rows(size):
        return pl.BlockSpec((part_block, size), lambda i: (i, 0))

    return pl.pallas_call(
        kernel,
        grid=(slots // part_block,),
        in_specs=[rows(x.shape[1]) for x in rowwise]
        + [pl.BlockSpec(x.shape, lambda i: (0, 0)) for x in matrices],
        out_specs=[rows(size) for size in sizes],
        out_shape=[jax.ShapeDtypeStruct((slots, size), bf16) for size in sizes],
    )(*rowwise, *matrices)


def on_device(
    resid_in,
    cotangent,
    norm_gain,
    routes,
    route_weights,
    gate_weight,
    up_weight,
    down_weight,
    out_weight,
    gate_b,
    gate_c,
    values_u,
    taps,
):
    token_count, model_width = resid_in.shape
    groups = lax.axis_size("sp")
    lanes = lax.axis_size("tp")
    lane = lax.axis_index("tp")
    expert_total = gate_weight.shape[0] * groups
    capacity = 4 * token_count // expert_total
    slots = expert_total * capacity
    quarter = model_width // lanes
    gate_mat, up_mat, down_mat = gate_weight[0], up_weight[0], down_weight[0]

    sent_rows, chooser, rank, high, low = chosen_rows(
        lane, routes, route_weights, resid_in, norm_gain, expert_total
    )
    got_part = exchanged(sent_rows.reshape(groups, capacity, quarter)).reshape(slots, quarter)
    sent_cots, token_chooser = weighted_rows(chooser, cotangent, rank, high, low)
    entry_cots = exchanged(sent_cots.reshape(groups, capacity, model_width))
    entry_cots = entry_cots.reshape(slots, model_width)
    entry_rows = placed_columns(lane, (got_part, ring_gather(got_part)), model_width)

    mixed = gate_c.astype(f32) * values_u.astype(f32)
    earlier = passed_along(mixed[-2:], "sp", 1)

    gate_pre = jnp.dot(entry_rows, gate_mat, preferred_element_type=f32)
    up_pre = jnp.dot(entry_rows, up_mat, preferred_element_type=f32)
    logistic = jax.nn.sigmoid(gate_pre)
    activated = gate_pre * logistic
    hidden = (activated * up_pre).astype(bf16)
    slope = up_pre * logistic * (1.0 + gate_pre * (1.0 - logistic))
    both_mat = jnp.concatenate([gate_mat, up_mat], axis=1)

    def weight_rows(further, first, count):
        at = ((lane + further) % lanes) * quarter + first * direct_width
        return lax.dynamic_slice_in_dim(both_mat, at, count * direct_width, axis=0)

    direct_mat = both_mat.reshape(lanes, quarter, -1)[:, -direct_width:]
    first_mat = jnp.concatenate(
        [weight_rows(2, 0, 2), weight_rows(3, 0, 2), weight_rows(1, 0, 2)]
        + [direct_mat.reshape(lanes * direct_width, -1)],
        axis=0,
    )
    other_mat = jnp.concatenate(
        [weight_rows(0, 0, 3), weight_rows(1, 2, 1), weight_rows(3, 2, 1), weight_rows(2, 2, 1)],
        axis=0,
    )
    activated, slope, hidden, first_mat, other_mat = lax.optimization_barrier(
        (activated.astype(bf16), slope.astype(bf16), hidden, first_mat, other_mat)
    )
    dboth, a_far, b_far, a_behind, b_behind, a_ahead, b_ahead, direct = by_rows(
        first_kernel,
        (entry_cots, activated, slope),
        (down_mat, first_mat),
        [both_mat.shape[1]] + [direct_width] * 6 + [lanes * direct_width],
    )

    def back(array):
        return exchanged(array.reshape(groups, capacity, -1)).reshape(slots, -1)

    def per_token(array):
        return jnp.dot(token_chooser, array, preferred_element_type=f32).astype(bf16)

    def plus(*arrays):
        return sum(array.astype(f32) for array in arrays).astype(bf16)

    a_far = turned(a_far, 1)
    b_far = turned(b_far, -1)
    direct = back(direct)
    a_next = turned(a_behind, -1)
    b_prev = turned(b_ahead, 1)
    a_prev = turned(plus(a_ahead, a_far), 1)
    b_next = turned(plus(b_behind, b_far), -1)
    wide_own, c_own, c_ahead, c_behind, c_far = by_rows(
        other_kernel,
        (dboth, a_next, b_prev),
        (other_mat,),
        [2 * direct_width] + [direct_width] * 4,
    )
    c_far = turned(c_far, 1)
    c_next = turned(c_behind, -1)
    c_ahead, direct = lax.optimization_barrier((c_ahead, direct))
    grad_down = jnp.einsum("rf,rd->fd", hidden, entry_cots, preferred_element_type=f32)
    (wide,) = by_rows(wide_kernel, (wide_own, a_prev, b_next), (), [2 * direct_width])
    c_own, wide = lax.optimization_barrier((c_own, wide))
    wide = back(wide)
    direct_parts = lane_gather(per_token(direct))
    c_prev = turned(plus(c_ahead, c_far), 1)
    narrow = back(plus(c_own, c_prev, c_next))
    wide_parts = lane_gather(per_token(wide))
    narrow_parts = lane_gather(per_token(narrow))
    pieces = (*wide_parts, *narrow_parts, *direct_parts)
    grad_resid = finish(lane, pieces, cotangent, resid_in, norm_gain)

    extended = jnp.concatenate([earlier, mixed], axis=0)
    conv = (
        taps[0] * extended[:token_count]
        + taps[1] * extended[1 : token_count + 1]
        + taps[2] * extended[2 : token_count + 2]
    )
    merged = (gate_b.astype(f32) * conv).astype(bf16)
    out_parts = jnp.einsum("td,tc->dc", grad_resid, merged, preferred_element_type=f32).astype(bf16)
    out_tiles = exchanged(out_parts.reshape(groups, model_width // groups, -1))
    grad_out_weight = jnp.sum(out_tiles.astype(f32), axis=0)
    late_both, out_parts = lax.optimization_barrier((dboth, out_parts))
    grad_both = jnp.einsum("rd,rf->df", entry_rows, late_both, preferred_element_type=f32)
    late_resid, grad_both = lax.optimization_barrier((grad_resid, grad_both))
    grad_gate, grad_up = jnp.split(grad_both, 2, axis=1)
    dmerged = jnp.dot(late_resid, out_weight, preferred_element_type=f32)
    grad_gate_b = (dmerged * conv).astype(bf16)
    dconv = dmerged * gate_b.astype(f32)
    later = passed_along(dconv[:2], "sp", -1)
    extended_grad = jnp.concatenate([dconv, later], axis=0)
    dmixed = (
        taps[2] * extended_grad[:token_count]
        + taps[1] * extended_grad[1 : token_count + 1]
        + taps[0] * extended_grad[2 : token_count + 2]
    )
    grad_gate_c = (dmixed * values_u.astype(f32)).astype(bf16)
    grad_values = (dmixed * gate_c.astype(f32)).astype(bf16)
    return (
        grad_gate[None],
        grad_up[None],
        grad_down[None],
        grad_resid,
        grad_out_weight,
        grad_gate_b,
        grad_gate_c,
        grad_values,
    )


def solution(mesh):
    placed = (
        P("sp", None),
        P("sp", None),
        P(),
        P("sp", None),
        P("sp", None),
        P("sp", None, "tp"),
        P("sp", None, "tp"),
        P("sp", "tp", None),
        P(None, "tp"),
        P("sp", "tp"),
        P("sp", "tp"),
        P("sp", "tp"),
        P(None, "tp"),
    )

    return jax.shard_map(
        on_device,
        mesh=mesh,
        in_specs=placed,
        out_specs=(
            P("sp", None, "tp"),
            P("sp", None, "tp"),
            P("sp", "tp", None),
            P("sp", None),
            P("sp", "tp"),
            P("sp", "tp"),
            P("sp", "tp"),
            P("sp", "tp"),
        ),
        check_vma=False,
    )
```
